128 devices in a mesh: kv: 16 (over z, x), tp: 8 (over y, core).
Axes of the slice: x: 4, y: 4, z: 4, core: 2. Of those that a mesh axis runs over, the one named last changes fastest.
Arguments:
- tokens: bfloat16 [768, 4096], P(None, ('kv', 'tp')), may hold values from -90 to 90
- norm_gain: float32 [4096], P('kv'), may hold values from 0.1 to 1.9
- w_query: bfloat16 [4096, 2048], P('kv', 'tp'), may hold values from -0.09375 to 0.09375
- w_key: bfloat16 [4096, 2048], P('kv', 'tp'), may hold values from -0.09375 to 0.09375
- w_value: bfloat16 [4096, 2048], P('kv', 'tp'), may hold values from -0.09375 to 0.09375
- w_outgate: bfloat16 [4096, 2048], P('kv', 'tp'), may hold values from -0.09375 to 0.09375
- w_igate: bfloat16 [4096, 16], replicated, may hold values from -0.09375 to 0.09375
- w_fgate: bfloat16 [4096, 16], replicated, may hold values from -0.09375 to 0.09375
- forget_bias: float32 [16], P('tp'), may hold values from -1 to 5
- head_gain: float32 [2048], P('tp'), may hold values from 0.1 to 1.9
- w_proj: bfloat16 [2048, 4096], P('tp', 'kv'), may hold values from -0.125 to 0.125
- mixer_gain: float32 [4096], P('kv'), may hold values from 0.1 to 1.9
- w_gate: bfloat16 [4096, 11264], P('kv', 'tp'), may hold values from -0.09375 to 0.09375
- w_up: bfloat16 [4096, 11264], P('kv', 'tp'), may hold values from -0.09375 to 0.09375
- w_down: bfloat16 [11264, 4096], P('tp', 'kv'), may hold values from -0.0546875 to 0.0546875
- state_c: float32 [768, 16, 128, 128], P('kv', 'tp'), may hold values from -0.5 to 0.5
- state_m: float32 [768, 16], P('kv', 'tp'), may hold values from -4 to 4
- tail_keys: bfloat16 [768, 16, 64, 128], P('kv', 'tp'), may hold values from -6 to 6
- tail_values: bfloat16 [768, 16, 64, 128], P('kv', 'tp'), may hold values from -6 to 6
- tail_gate: float32 [768, 16, 64], P('kv', 'tp'), may hold values from -8 to 130
- block_forget: float32 [768, 16], P('kv', 'tp'), may hold values from -6 to 0
- lengths: int32 [768], P('kv'), may hold values from 1 to 64, 12288 in all
Outputs:
- result: bfloat16 [768, 4096], P(None, ('kv', 'tp'))
The draws below stay inside these ranges and needn't reach their ends.
All inputs are finite; a program needn't handle non-finite values. No bound on the sum of `lengths` on one device may be relied on, other than what follows from the above.
Results may differ from the reference program's by a relative error of at most 0.012.
Values may be sent and summed in bfloat16 or wider, within the bound.
A program may use at most 128 MiB of HBM per device.

```python
import math
import jax
import jax.numpy as jnp
import numpy as np
from jax import lax

D = 4096
HEADS = 16
DH = 128
FF = 11264
SPAN = 64
SEQS = 768
N_TP = 8


def draw_tokens(key, part):
    first, second = jax.random.split(key, 2)
    columns = jnp.arange(D, dtype=jnp.float32) / D
    rough = jax.random.uniform(second, (D,), jnp.float32, 0.6, 1.6)
    scale = 0.4 * 10.0 ** columns * rough
    base = jnp.clip(jax.random.normal(first, (SEQS, D), jnp.float32), -4.0, 4.0)
    values = base * scale
    return values.astype(jnp.bfloat16)


def draw_tail_gate(key, part):
    first = jax.random.fold_in(key, 0)
    base = jnp.clip(jax.random.normal(first, (SEQS, HEADS, SPAN), jnp.float32) * 1.5 - 1.0, -8.0, 6.0)
    return base


def shard_levels(own_key, extent, shards, smallest, high):
    gain, own = 1.0, jax.random.fold_in(own_key, 6)
    for dim, shards_of in shards:
        steps = jnp.exp(jax.random.uniform(jax.random.fold_in(own, dim), (shards_of,), jnp.float32, smallest / len(shards), high / len(shards)))
        gain = gain * jnp.repeat(steps, extent[dim] // shards_of).reshape([-1 if axis == dim else 1 for axis in range(len(extent))])
    return gain


def length_profile(count, total, limit, lean):
    weights = [(1 << 20) // math.isqrt(rank ** lean) + 1 for rank in range(2, count + 1)]
    surplus, counts = total - limit - (count - 1), [1] * (count - 1)
    while surplus > 0:
        candidates = [i for i in range(count - 1) if counts[i] < limit]
        pool, left = sum([weights[i] for i in candidates]), surplus
        for i in candidates:
            more = min(limit - counts[i], max(1, left * weights[i] // pool), surplus)
            counts[i] = counts[i] + more
            surplus = surplus - more
    return np.array([limit] + counts)


def uneven_parts(own_key, count, total, limit, lean):
    if count == 2:
        one = jax.random.randint(own_key, (), max(1, total - limit), min(limit, total - 1) + 1)
        return jnp.stack([one, total - one])
    sizes = jnp.asarray(length_profile(count, total, limit, lean), jnp.int32)
    twos = (count - 1) // 2
    giver, taker = sizes[1:1 + 2 * twos:2], sizes[2:2 + 2 * twos:2]
    room = jnp.minimum(giver - 1, limit - taker)
    moved = jax.random.randint(jax.random.fold_in(own_key, 1), (twos,), 0, 1 << 20) % (room + 1)
    sizes = sizes.at[1:1 + 2 * twos:2].set(giver - moved).at[2:2 + 2 * twos:2].set(taker + moved)
    return sizes[jax.random.permutation(jax.random.fold_in(own_key, 2), count)]


def bell_draw(key, shape, spread, bound, pieces=(), kind=jnp.bfloat16):
    entries = spread * jax.random.normal(key, shape, jnp.float32)
    if pieces:
        entries = entries * shard_levels(key, shape, pieces, -0.22, 0.18)
    return jnp.clip(entries, -bound, bound).astype(kind)


def setup_inputs(seed: int = 0) -> dict:
    arg_keys = jax.random.split(jax.random.key(seed), 23)
    tokens = draw_tokens(jax.random.fold_in(arg_keys[22], 71), 0)
    norm_gain = jnp.clip(1.0 + 0.18 * jax.random.normal(arg_keys[1], (D,), jnp.float32), 0.1, 1.9)
    w_query = bell_draw(arg_keys[2], (D, HEADS * DH), D ** -0.5, 0.09375, ((0, 16), (1, 8)))
    w_key = bell_draw(arg_keys[3], (D, HEADS * DH), D ** -0.5, 0.09375, ((0, 16), (1, 8)))
    w_value = bell_draw(arg_keys[4], (D, HEADS * DH), D ** -0.5, 0.09375, ((0, 16), (1, 8)))
    w_outgate = bell_draw(arg_keys[5], (D, HEADS * DH), D ** -0.5, 0.09375, ((0, 16), (1, 8)))
    w_igate = bell_draw(arg_keys[6], (D, HEADS), D ** -0.5, 0.09375)
    w_fgate = bell_draw(arg_keys[7], (D, HEADS), D ** -0.5, 0.09375)
    forget_bias = jnp.clip(-1.0 + 6.0 * jax.random.uniform(arg_keys[8], (HEADS,), jnp.float32) ** shard_levels(arg_keys[8], (HEADS,), ((0, 8),), -0.2, 0.2), -1.0, 5.0)
    head_gain = jnp.clip(1.0 + 0.18 * jax.random.normal(arg_keys[9], (HEADS * DH,), jnp.float32), 0.1, 1.9)
    w_proj = bell_draw(arg_keys[10], (HEADS * DH, D), (HEADS * DH) ** -0.5, 0.125, ((0, 8), (1, 16)))
    mixer_gain = jnp.clip(1.0 + 0.18 * jax.random.normal(arg_keys[11], (D,), jnp.float32), 0.1, 1.9)
    w_gate = bell_draw(arg_keys[12], (D, FF), D ** -0.5, 0.09375, ((0, 16), (1, 8)))
    w_up = bell_draw(arg_keys[13], (D, FF), D ** -0.5, 0.09375, ((0, 16), (1, 8)))
    w_down = bell_draw(arg_keys[14], (FF, D), FF ** -0.5, 0.0546875, ((0, 8), (1, 16)))
    state_c = bell_draw(arg_keys[15], (SEQS, HEADS, DH, DH), DH ** -0.5, 0.5, ((0, 16), (1, 8)), jnp.float32)
    state_m = bell_draw(arg_keys[16], (SEQS, HEADS), 1.0, 4.0, ((0, 16), (1, 8)), jnp.float32)
    tail_keys = bell_draw(arg_keys[17], (SEQS, HEADS, SPAN, DH), 1.0, 6.0, ((0, 16), (1, 8)))
    tail_values = bell_draw(arg_keys[18], (SEQS, HEADS, SPAN, DH), 1.0, 6.0, ((0, 16), (1, 8)))
    tail_gate = draw_tail_gate(jax.random.fold_in(arg_keys[22], 71), 0)
    block_forget = jnp.clip(-6.0 + 6.0 * jax.random.uniform(arg_keys[20], (SEQS, HEADS), jnp.float32) ** shard_levels(arg_keys[20], (SEQS, HEADS), ((0, 16), (1, 8)), -0.2, 0.2), -6.0, 0.0)
    lengths = uneven_parts(arg_keys[21], SEQS, SEQS * SPAN // 4, SPAN, 2).astype(jnp.int32)
    return dict(tokens=tokens, norm_gain=norm_gain, w_query=w_query, w_key=w_key, w_value=w_value, w_outgate=w_outgate, w_igate=w_igate, w_fgate=w_fgate, forget_bias=forget_bias, head_gain=head_gain, w_proj=w_proj, mixer_gain=mixer_gain, w_gate=w_gate, w_up=w_up, w_down=w_down, state_c=state_c, state_m=state_m, tail_keys=tail_keys, tail_values=tail_values, tail_gate=tail_gate, block_forget=block_forget, lengths=lengths)


EPS = 1e-06

def recall(query, key, value, igate, fpre, state_c, state_m, tail_keys, tail_values, tail_gate, block_forget, lengths):
    f32 = jnp.float32
    span = tail_keys.shape[2]
    head_dim = query.shape[2]
    running = block_forget + jax.nn.log_sigmoid(fpre)
    inter = running + state_m
    live = jnp.arange(span, dtype=jnp.int32)[None, :] < lengths[:, None]
    tail_log = jnp.where(live[:, None, :], running[:, :, None] + tail_gate, -jnp.inf)
    top = jnp.maximum(jnp.maximum(inter, lax.optimization_barrier(jnp.max(tail_log, axis=2))), igate)
    w_inter = jnp.exp(inter - top)
    w_tail = jnp.exp(tail_log - top[:, :, None])
    w_own = jnp.exp(igate - top)
    scores = jnp.einsum('shpd,shd->shp', tail_keys.astype(f32), query) * head_dim ** (-0.5)
    own = lax.optimization_barrier(jnp.sum(query * key, axis=2))
    memory = jnp.einsum('shvk,shk->shv', state_c, query)
    weighted = w_tail * scores
    return w_inter[:, :, None] * memory + jnp.einsum('shp,shpv->shv', weighted, tail_values.astype(f32)) + (w_own * own)[:, :, None] * value

def rounded_parts(left, right, groups):
    f32 = jnp.float32
    rows = left.shape[0]
    inner = left.shape[1] // groups
    parts = jnp.einsum('sgc,gcd->sgd', left.reshape(rows, groups, inner).astype(f32), right.reshape(groups, inner, right.shape[1]).astype(f32))
    parts = lax.optimization_barrier(parts.astype(jnp.bfloat16))
    return lax.optimization_barrier(jnp.sum(parts.astype(f32), axis=1))

def reference(tokens, norm_gain, w_query, w_key, w_value, w_outgate, w_igate, w_fgate, forget_bias, head_gain, w_proj, mixer_gain, w_gate, w_up, w_down, state_c, state_m, tail_keys, tail_values, tail_gate, block_forget, lengths):
    f32 = jnp.float32
    bf = jnp.bfloat16
    seqs = tokens.shape[0]
    xf = tokens.astype(f32)
    inv_first = lax.rsqrt(lax.optimization_barrier(jnp.mean(xf * xf, axis=1, keepdims=True)) + EPS)
    scaled = (xf * norm_gain).astype(bf)

    def project(weight):
        return jnp.dot(scaled, weight, preferred_element_type=f32) * inv_first
    query = project(w_query).reshape(seqs, HEADS, DH)
    key = project(w_key).reshape(seqs, HEADS, DH) * DH ** (-0.5)
    value = project(w_value).reshape(seqs, HEADS, DH)
    outgate = project(w_outgate)
    igate = project(w_igate)
    fpre = project(w_fgate) + forget_bias
    recalled = recall(query, key, value, igate, fpre, state_c, state_m, tail_keys, tail_values, tail_gate, block_forget, lengths)
    normed = recalled * lax.rsqrt(lax.optimization_barrier(jnp.mean(recalled * recalled, axis=2, keepdims=True)) + EPS)
    mixed = (normed.reshape(seqs, HEADS * DH) * head_gain * jax.nn.sigmoid(outgate)).astype(bf)
    attended = rounded_parts(mixed, w_proj, N_TP)
    middle = (xf + attended).astype(bf)
    middlef = middle.astype(f32)
    inv_second = lax.rsqrt(lax.optimization_barrier(jnp.mean(middlef * middlef, axis=1, keepdims=True)) + EPS)
    scaled_mid = (middlef * mixer_gain).astype(bf)
    gate = jnp.dot(scaled_mid, w_gate, preferred_element_type=f32) * inv_second
    up = jnp.dot(scaled_mid, w_up, preferred_element_type=f32) * inv_second
    hidden = (jax.nn.silu(gate) * up).astype(bf)
    mixed_out = rounded_parts(hidden, w_down, N_TP)
    return (middlef + mixed_out).astype(bf)
```

```python
import jax
import jax.numpy as jnp
from jax import lax
from jax.experimental import pallas as pl
from jax.experimental.pallas import tpu as pltpu
from jax.sharding import PartitionSpec as P

D = 4096
EPS = 1e-06
F32 = jnp.float32
BF = jnp.bfloat16
MESH = pl.DeviceIdType.MESH
N1 = 1024
N2 = 2816
FFD = 1408


def remote(src, dst, ss, rs, dev):
    return pltpu.make_async_remote_copy(
        src_ref=src, dst_ref=dst, send_sem=ss, recv_sem=rs, device_id=dev, device_id_type=MESH
    )


def mod4(v):
    return lax.rem(v, 4)


def transpose_padded(rows):
    missing = 128 - rows.shape[0]
    if missing:
        rows = jnp.concatenate([rows, jnp.zeros((missing, rows.shape[1]), F32)], axis=0)
    return rows.T


def column_of(row):
    return jnp.broadcast_to(row, (128, 128)).T


def layer(
    tokens, norm_gain, w_query, w_key, w_value, w_outgate, w_igate, w_fgate, head_gain, w_proj,
    mixer_gain, w_gate, w_up, w_down, state_c, tail_keys, tail_values, tail_gate, meta,
    out,
    tok_v, wide_t, wide, scaled, wqkvo, wig_v, wfg_v, wproj_v, wgu, wdown_v, cbuf, kbuf, vbuf,
    gsend, grecv,
    a_p, a_own, a_in, a_comb, a_l, a_r, a_q, a_qin, a_qcomb, a_ql, a_qr,
    qs, tailo, mix_all, att_send, att_recv, mid_all, scaled_mid, ssend, srecv, mid_sel,
    b_p, b_own, b_in, b_comb, b_l, b_r, b_q, b_qin, b_qcomb, b_ql, b_qr,
    hid, fsend, frecv,
    lsem, tok_s, tok_r, g_s, g_r, mix_s, mix_r, att_s, att_r, mid_s, mid_r, sq_s, sq_r,
    ra_s, ra_r, rb_s, rb_r, h_s, h_r, f_s, f_r,
):
    kv = lax.axis_index("kv")
    tp = lax.axis_index("tp")
    z = lax.div(kv, 4)
    x = lax.rem(kv, 4)
    c = lax.rem(tp, 2)
    pa = x * (1 - c) + z * c
    pb = z * (1 - c) + x * c

    def kv_of(ia, ib):
        return ia * (1 + 3 * c) + ib * (4 - 3 * c)

    def at_a(g):
        return (kv_of(mod4(pa + g), pb), tp)

    def at_b(g):
        return (kv_of(pa, mod4(pb + g)), tp)

    def kv_peer(i):
        return mod4(z + i // 4) * 4 + mod4(x + i % 4)

    def kv_from(i):
        return mod4(z + 4 - i // 4) * 4 + mod4(x + 4 - i % 4)

    def tp_peer(r):
        return lax.rem(tp + r, 8)

    def tp_from(r):
        return lax.rem(tp + 8 - r, 8)

    def rows48(k):
        return pl.ds(pl.multiple_of(k * 48, 16), 48)

    def rows96(k):
        return pl.ds(pl.multiple_of(k * 96, 32), 96)

    def rows32(k):
        return pl.ds(pl.multiple_of(k * 32, 32), 32)

    sends = []

    def send(*args):
        copy = remote(*args)
        copy.start()
        sends.append(copy)

    loads = [
        pltpu.make_async_copy(tokens, tok_v, lsem.at[0]),
        pltpu.make_async_copy(w_query, wqkvo.at[:, pl.ds(0, 256)], lsem.at[1]),
        pltpu.make_async_copy(w_key, wqkvo.at[:, pl.ds(256, 256)], lsem.at[2]),
        pltpu.make_async_copy(w_value, wqkvo.at[:, pl.ds(512, 256)], lsem.at[3]),
        pltpu.make_async_copy(w_outgate, wqkvo.at[:, pl.ds(768, 256)], lsem.at[4]),
        pltpu.make_async_copy(w_igate.at[pl.ds(pl.multiple_of(kv * 256, 256), 256)], wig_v, lsem.at[5]),
        pltpu.make_async_copy(w_fgate.at[pl.ds(pl.multiple_of(kv * 256, 256), 256)], wfg_v, lsem.at[6]),
        pltpu.make_async_copy(state_c, cbuf, lsem.at[7]),
        pltpu.make_async_copy(tail_keys, kbuf, lsem.at[8]),
        pltpu.make_async_copy(tail_values, vbuf, lsem.at[9]),
        pltpu.make_async_copy(w_proj, wproj_v, lsem.at[10]),
        pltpu.make_async_copy(w_gate, wgu.at[:, pl.ds(0, FFD)], lsem.at[11]),
        pltpu.make_async_copy(w_up, wgu.at[:, pl.ds(FFD, FFD)], lsem.at[12]),
        pltpu.make_async_copy(w_down, wdown_v, lsem.at[13]),
    ]
    for load in loads:
        load.start()

    barrier = pltpu.get_barrier_semaphore()
    for i in range(1, 16):
        pl.semaphore_signal(barrier, inc=1, device_id=(kv_peer(i), tp), device_id_type=MESH)
    for r in range(1, 8):
        pl.semaphore_signal(barrier, inc=1, device_id=(kv, tp_peer(r)), device_id_type=MESH)

    loads[0].wait()
    tok_f = tok_v[...].astype(F32)
    wide_t[rows32(tp), :] = tok_f.T.astype(BF)
    pl.semaphore_wait(barrier, 22)

    for r in range(1, 8):
        mine = wide_t.at[rows32(tp)]
        send(mine, mine, tok_s.at[r], tok_r.at[r], (kv, tp_peer(r)))

    lane = lax.broadcasted_iota(jnp.int32, (128, 128), 1)
    for i in range(5, 7):
        loads[i].wait()
    grow = lax.broadcasted_iota(jnp.int32, (16, 128), 0)
    glane = lax.broadcasted_iota(jnp.int32, (16, 128), 1)
    pick_i = jnp.where((glane < 2) & (grow == 2 * tp + glane), 1.0, 0.0).astype(BF)
    pick_f = jnp.where((glane >= 2) & (glane < 4) & (grow == 2 * tp + glane - 2), 1.0, 0.0).astype(BF)
    gate_w = (
        jnp.dot(wig_v[...], pick_i, preferred_element_type=F32)
        + jnp.dot(wfg_v[...], pick_f, preferred_element_type=F32)
    ).astype(BF)
    forget_row = meta[0:1, :]
    state_row = meta[1:2, :]
    length_row = meta[2:3, :]
    bias_row = meta[3:4, :]
    tg = transpose_padded(tail_gate[...])
    lane64 = lax.broadcasted_iota(jnp.int32, (64, 128), 1)
    gate_t = jnp.where(lane64 < 64, tg[:64], pltpu.roll(tg[64:], 64, 1))

    for r in range(1, 8):
        src = wide_t.at[rows32(tp_from(r))]
        remote(src, src, tok_s.at[r], tok_r.at[r], (kv, tp)).wait_recv()
    for b in range(6):
        block = wide_t[:, 128 * b : 128 * b + 128].astype(F32).T
        wide[128 * b : 128 * b + 128, :] = block.astype(BF)
        scaled[128 * b : 128 * b + 128, :] = (block * norm_gain[...]).astype(BF)

    def ring_sum(lhs, weights, n, tile, p, own, inn, comb, from_l, from_r, q, qin, qcomb, ql, qr, ss, rs, between):
        half = n // 2
        first, second = pl.ds(0, half), pl.ds(half, half)

        def group(g, put):
            ia = mod4(pa + g)
            rows = jnp.concatenate([lhs[rows48(kv_of(ia, ib)), :] for ib in range(4)], axis=0)

            def step(t, _):
                cols = pl.ds(pl.multiple_of(t * tile, tile), tile)
                put(cols, jnp.dot(rows, weights[:, cols], preferred_element_type=F32))
                return 0

            lax.fori_loop(0, n // tile, step, 0)

        def into(ref):
            def put(cols, value):
                ref[:, cols] = value.astype(ref.dtype)

            return put

        def add_rows(count, fn):
            def step(i, _):
                fn(pl.ds(pl.multiple_of(i * 16, 16), 16))
                return 0

            lax.fori_loop(0, count // 16, step, 0)

        def waited(dst, i):
            remote(dst, dst, ss.at[i], rs.at[i], (kv, tp)).wait_recv()

        right, left = at_a(1), at_a(3)
        group(2, into(p.at[0]))
        send(p.at[0, :, first], inn.at[0], ss.at[0], rs.at[0], right)
        send(p.at[0, :, second], inn.at[1], ss.at[1], rs.at[1], left)
        group(1, into(p.at[1]))
        send(p.at[1, :, second], from_l.at[:, second], ss.at[2], rs.at[2], right)
        group(3, into(p.at[2]))
        send(p.at[2, :, first], from_r.at[:, first], ss.at[3], rs.at[3], left)
        group(0, into(own))
        between()
        waited(inn.at[0], 0)

        def comb0(rows):
            comb[0, rows, :] = (p[1, rows, first].astype(F32) + inn[0, rows, :].astype(F32)).astype(BF)

        add_rows(192, comb0)
        send(comb.at[0], from_l.at[:, first], ss.at[4], rs.at[4], right)
        waited(inn.at[1], 1)

        def comb1(rows):
            comb[1, rows, :] = (p[2, rows, second].astype(F32) + inn[1, rows, :].astype(F32)).astype(BF)

        add_rows(192, comb1)
        send(comb.at[1], from_r.at[:, second], ss.at[5], rs.at[5], left)
        waited(from_l.at[:, second], 2)
        waited(from_r.at[:, first], 3)
        waited(from_l.at[:, first], 4)
        waited(from_r.at[:, second], 5)

        right, left = at_b(1), at_b(3)

        def total(g, put):
            base = mod4(pb + g) * 48
            for i in range(3):
                rows = pl.ds(pl.multiple_of(base + 16 * i, 16), 16)
                put(
                    pl.ds(16 * i, 16),
                    own[rows, :] + from_l[rows, :].astype(F32) + from_r[rows, :].astype(F32),
                )

        def into_q(j):
            def put(rows, value):
                q[j, rows, :] = value.astype(BF)

            return put

        total(2, into_q(0))
        send(q.at[0, :, first], qin.at[0], ss.at[6], rs.at[6], right)
        send(q.at[0, :, second], qin.at[1], ss.at[7], rs.at[7], left)
        total(1, into_q(1))
        send(q.at[1, :, second], ql.at[:, second], ss.at[8], rs.at[8], right)
        total(3, into_q(2))
        send(q.at[2, :, first], qr.at[:, first], ss.at[9], rs.at[9], left)
        waited(qin.at[0], 6)
        qcomb[0] = (q[1, :, first].astype(F32) + qin[0].astype(F32)).astype(BF)
        send(qcomb.at[0], ql.at[:, first], ss.at[10], rs.at[10], right)
        waited(qin.at[1], 7)
        qcomb[1] = (q[2, :, second].astype(F32) + qin[1].astype(F32)).astype(BF)
        send(qcomb.at[1], qr.at[:, second], ss.at[11], rs.at[11], left)
        mine = pl.ds(pl.multiple_of(pb * 48, 16), 48)
        waited(ql.at[:, second], 8)
        waited(qr.at[:, first], 9)
        waited(ql.at[:, first], 10)
        waited(qr.at[:, second], 11)

        def result(cols):
            return (
                own[mine, cols]
                + from_l[mine, cols].astype(F32)
                + from_r[mine, cols].astype(F32)
                + ql[:, cols].astype(F32)
                + qr[:, cols].astype(F32)
            )

        return result

    def small_sum(recv_ref, own_tile, ss, rs):
        acc = own_tile
        for i in range(1, 16):
            remote(recv_ref.at[i], recv_ref.at[i], ss.at[i], rs.at[i], (kv, tp)).wait_recv()
            acc = acc + recv_ref[i]
        return acc

    lane48 = lax.broadcasted_iota(jnp.int32, (48, 128), 1)

    def gate_tiles():
        def step(k, _):
            rows = rows48(k)
            part = jnp.dot(scaled[rows, :], gate_w, preferred_element_type=F32)
            wf = wide[rows, :].astype(F32)
            sq = jnp.sum(wf * wf, axis=1, keepdims=True)
            gsend[k] = transpose_padded(jnp.where(lane48 == 4, sq, part))[:8]
            return 0

        lax.fori_loop(0, 16, step, 0)
        for i in range(1, 16):
            k = kv_peer(i)
            send(gsend.at[k], grecv.at[i], g_s.at[i], g_r.at[i], (k, tp))

    for i in range(1, 5):
        loads[i].wait()
    proj = ring_sum(
        scaled, wqkvo, N1, 256, a_p, a_own, a_in, a_comb, a_l, a_r, a_q, a_qin, a_qcomb, a_ql, a_qr,
        ra_s, ra_r, gate_tiles,
    )
    gsum = small_sum(grecv, gsend[kv], g_s, g_r)
    inv_row = lax.rsqrt(gsum[4:5, :] / D + EPS)
    inv_col = column_of(inv_row)[:48]
    lane8 = lax.broadcasted_iota(jnp.int32, (8, 128), 1)

    def pair_row(first, second):
        a8 = jnp.broadcast_to(first, (8, 128))
        b8 = jnp.broadcast_to(second, (8, 128))
        return jnp.where(lane8 < 64, a8, pltpu.roll(b8, 64, 1))

    igate = pair_row(gsum[0:1, :] * inv_row, gsum[1:2, :] * inv_row)
    fpre = pair_row(gsum[2:3, :] * inv_row, gsum[3:4, :] * inv_row) + bias_row
    log_sig = -(jnp.maximum(-fpre, 0.0) + jnp.log1p(jnp.exp(-jnp.abs(fpre))))
    running = forget_row + log_sig
    inter = running + state_row
    pos = lax.broadcasted_iota(jnp.int32, (64, 128), 0).astype(F32)
    tail_log = jnp.where(pos < length_row, running[0:1] + gate_t, -jnp.inf)
    top = jnp.maximum(jnp.maximum(inter[0:1], jnp.max(tail_log, axis=0, keepdims=True)), igate[0:1])
    w_inter = jnp.exp(inter[0:1] - top)
    w_own = column_of(jnp.exp(igate[0:1] - top))
    w_tail = jnp.exp(tail_log - top)

    for h in range(2):
        qs[h] = proj(pl.ds(128 * h, 128)) * inv_col
    for i in range(7, 10):
        loads[i].wait()

    def recall_step(s, carry):
        mem_t, sc_t = carry
        for h in range(2):
            qrow = qs[h, pl.ds(s, 1), :]
            m = jnp.sum(cbuf[s, h] * qrow, axis=1, keepdims=True)
            mem_t = jnp.where(lane == 64 * h + s, m, mem_t)
            sc = jnp.sum(kbuf[s, h].astype(F32) * qrow, axis=1, keepdims=True)
            sc_t = jnp.where(lane64 == 64 * h + s, sc, sc_t)
        return mem_t, sc_t

    mem_t, sc_t = lax.fori_loop(
        0, 48, recall_step, (jnp.zeros((128, 128), F32), jnp.zeros((64, 128), F32))
    )
    weighted = w_tail * (sc_t * 128 ** (-0.5))

    def tail_step(s, _):
        for h in range(2):
            wcol = jnp.sum(jnp.where(lane64 == 64 * h + s, weighted, 0.0), axis=1, keepdims=True)
            tailo[h, pl.ds(s, 1), :] = jnp.sum(vbuf[s, h].astype(F32) * wcol, axis=0, keepdims=True)
        return 0

    lax.fori_loop(0, 48, tail_step, 0)
    memory = (mem_t * w_inter).T
    mixed = []
    for h in range(2):
        q = qs[h]
        k = proj(pl.ds(256 + 128 * h, 128)) * inv_col * 128 ** (-0.5)
        v = proj(pl.ds(512 + 128 * h, 128)) * inv_col
        og = proj(pl.ds(768 + 128 * h, 128)) * inv_col
        own = jnp.sum(q * k, axis=1, keepdims=True)
        recalled = memory[64 * h : 64 * h + 48] + tailo[h] + w_own[64 * h : 64 * h + 48] * own * v
        ms = jnp.mean(recalled * recalled, axis=1, keepdims=True)
        normed = recalled * lax.rsqrt(ms + EPS)
        hg = head_gain[:, 128 * h : 128 * h + 128]
        mixed.append((normed * hg * (1.0 / (1.0 + jnp.exp(-og)))).astype(BF))
    mix_all[rows48(kv), :] = jnp.concatenate(mixed, axis=1)
    for i in range(1, 16):
        mine = mix_all.at[rows48(kv)]
        send(mine, mine, mix_s.at[i], mix_r.at[i], (kv_peer(i), tp))
    loads[10].wait()
    for i in range(1, 16):
        src = mix_all.at[rows48(kv_from(i))]
        remote(src, src, mix_s.at[i], mix_r.at[i], (kv, tp)).wait_recv()

    for r in [4, 3, 5, 2, 6, 1, 7, 0]:
        part = jnp.dot(mix_all[rows96(tp_peer(r)), :], wproj_v[...], preferred_element_type=F32)
        att_send[r] = part.astype(BF)
        if r:
            send(att_send.at[r], att_recv.at[r], att_s.at[r], att_r.at[r], (kv, tp_peer(r)))
    attended = att_send[0].astype(F32)
    for r in range(1, 8):
        remote(att_recv.at[r], att_recv.at[r], att_s.at[r], att_r.at[r], (kv, tp)).wait_recv()
        attended = attended + att_recv[r].astype(F32)
    mid_all[rows96(tp), :] = (wide[rows96(tp), :].astype(F32) + attended).astype(BF)
    for r in [4, 3, 5, 2, 6, 1, 7]:
        mine = mid_all.at[rows96(tp)]
        send(mine, mine, mid_s.at[r], mid_r.at[r], (kv, tp_peer(r)))
    for r in range(1, 8):
        src = mid_all.at[rows96(tp_from(r))]
        remote(src, src, mid_s.at[r], mid_r.at[r], (kv, tp)).wait_recv()

    def scale_mid(k, _):
        rows = rows48(k)
        m = mid_all[rows, :].astype(F32)
        scaled_mid[rows, :] = (m * mixer_gain[...]).astype(BF)
        return 0

    lax.fori_loop(0, 16, scale_mid, 0)

    def square_tiles():
        def step(k, _):
            m = mid_all[rows48(k), :].astype(F32)
            sq = m * m
            row = jnp.sum(transpose_padded(sq[:, :128] + sq[:, 128:]), axis=0, keepdims=True)
            ssend[k] = jnp.broadcast_to(row, (8, 128))
            return 0

        lax.fori_loop(0, 16, step, 0)
        for i in range(1, 16):
            k = kv_peer(i)
            send(ssend.at[k], srecv.at[i], sq_s.at[i], sq_r.at[i], (k, tp))
        srow = lax.broadcasted_iota(jnp.int32, (256, 128), 0)
        slane = lax.broadcasted_iota(jnp.int32, (256, 128), 1)
        pick = jnp.where((slane < 32) & (srow == 32 * tp + slane), 1.0, 0.0).astype(BF)
        mid_sel[...] = jnp.dot(mid_all[...], pick, preferred_element_type=F32)

    loads[11].wait()
    loads[12].wait()
    both = ring_sum(
        scaled_mid, wgu, N2, 256, b_p, b_own, b_in, b_comb, b_l, b_r, b_q, b_qin, b_qcomb, b_ql, b_qr,
        rb_s, rb_r, square_tiles,
    )
    ssum = small_sum(srecv, ssend[kv], sq_s, sq_r)
    inv_mid = column_of(lax.rsqrt(ssum[0:1] / D + EPS))[:48]

    def hidden_step(t, _):
        cols = pl.ds(pl.multiple_of(t * 128, 128), 128)
        gate = both(cols) * inv_mid
        up = both(pl.ds(pl.multiple_of(t * 128 + FFD, 128), 128)) * inv_mid
        hid[rows48(kv), cols] = (gate * (1.0 / (1.0 + jnp.exp(-gate))) * up).astype(BF)
        return 0

    lax.fori_loop(0, FFD // 128, hidden_step, 0)

    part_rows = (pl.ds(0, 32), pl.ds(32, 16))

    def chunk(ra, rb):
        return hid.at[rows48(kv_of(mod4(pa + 4 - ra), mod4(pb + 4 - rb)))]

    def piece(ref, i):
        return ref.at[part_rows[i]]

    def hop(ref, i, dev):
        send(ref, ref, h_s.at[i], h_r.at[i], dev)

    def arrived(ref, i):
        remote(ref, ref, h_s.at[i], h_r.at[i], (kv, tp)).wait_recv()

    def spread(rb):
        hop(chunk(0, rb), 4 + rb, at_a(1))
        hop(chunk(0, rb), 8 + rb, at_a(3))

    hop(chunk(0, 0), 0, at_b(1))
    hop(chunk(0, 0), 1, at_b(3))
    spread(0)
    arrived(chunk(0, 1), 0)
    hop(piece(chunk(0, 1), 0), 2, at_b(1))
    spread(1)
    arrived(chunk(0, 3), 1)
    hop(piece(chunk(0, 3), 1), 3, at_b(3))
    spread(3)
    arrived(chunk(1, 0), 4)
    hop(chunk(1, 0), 12, at_a(1))
    arrived(piece(chunk(0, 2), 0), 2)
    arrived(piece(chunk(0, 2), 1), 3)
    spread(2)
    arrived(chunk(1, 1), 5)
    hop(chunk(1, 1), 13, at_a(1))
    arrived(chunk(3, 3), 11)
    hop(chunk(3, 3), 15, at_a(3))
    arrived(chunk(3, 2), 10)
    hop(chunk(3, 2), 14, at_a(3))
    loads[13].wait()
    arrived(chunk(1, 2), 6)
    arrived(chunk(1, 3), 7)
    arrived(chunk(3, 0), 8)
    arrived(chunk(3, 1), 9)
    for rb in range(4):
        arrived(chunk(2, rb), 12 + rb)

    for b in range(6):
        part = jnp.dot(hid[128 * b : 128 * b + 128, :], wdown_v[...], preferred_element_type=F32)
        fsend[:, 128 * b : 128 * b + 128] = part.T.astype(BF)
    for r in [4, 3, 5, 2, 6, 1, 7]:
        t = tp_peer(r)
        send(fsend.at[rows32(t)], frecv.at[r], f_s.at[r], f_r.at[r], (kv, t))
    total = fsend[rows32(tp), :].astype(F32)
    for r in range(1, 8):
        remote(frecv.at[r], frecv.at[r], f_s.at[r], f_r.at[r], (kv, tp)).wait_recv()
        total = total + frecv[r].astype(F32)
    for b in range(6):
        down = transpose_padded(total[:, 128 * b : 128 * b + 128])
        rows = slice(128 * b, 128 * b + 128)
        out[rows, :] = (mid_sel[rows, :] + down)[:, :32].astype(BF)
    for copy in sends:
        copy.wait_send()


def per_device(
    tokens, norm_gain, w_query, w_key, w_value, w_outgate, w_igate, w_fgate, forget_bias, head_gain,
    w_proj, mixer_gain, w_gate, w_up, w_down, state_c, state_m, tail_keys, tail_values, tail_gate,
    block_forget, lengths,
):
    def pair_row(a):
        return jnp.pad(a.T, ((0, 0), (0, 16))).reshape(1, 128)

    length_row = pair_row(jnp.broadcast_to(lengths.astype(F32)[:, None], (48, 2)))
    bias_row = pair_row(jnp.broadcast_to(forget_bias[None, :], (48, 2)))
    meta = jnp.concatenate(
        [pair_row(block_forget), pair_row(state_m), length_row, bias_row, jnp.zeros((4, 128), F32)], axis=0
    )
    any_spec = pl.BlockSpec(memory_space=pl.ANY)
    vm_spec = pl.BlockSpec(memory_space=pltpu.VMEM)
    dma = pltpu.SemaphoreType.DMA

    def ring_bufs(n):
        return [
            pltpu.VMEM((3, 192, n), BF),
            pltpu.VMEM((192, n), F32),
            pltpu.VMEM((2, 192, n // 2), BF),
            pltpu.VMEM((2, 192, n // 2), BF),
            pltpu.VMEM((192, n), BF),
            pltpu.VMEM((192, n), BF),
            pltpu.VMEM((3, 48, n), BF),
            pltpu.VMEM((2, 48, n // 2), BF),
            pltpu.VMEM((2, 48, n // 2), BF),
            pltpu.VMEM((48, n), BF),
            pltpu.VMEM((48, n), BF),
        ]

    scratch = [
        pltpu.VMEM((768, 32), BF),
        pltpu.VMEM((256, 768), BF),
        pltpu.VMEM((768, 256), BF),
        pltpu.VMEM((768, 256), BF),
        pltpu.VMEM((256, N1), BF),
        pltpu.VMEM((256, 16), BF),
        pltpu.VMEM((256, 16), BF),
        pltpu.VMEM((256, 256), BF),
        pltpu.VMEM((256, N2), BF),
        pltpu.VMEM((FFD, 256), BF),
        pltpu.VMEM((48, 2, 128, 128), F32),
        pltpu.VMEM((48, 2, 64, 128), BF),
        pltpu.VMEM((48, 2, 64, 128), BF),
        pltpu.VMEM((16, 8, 128), F32),
        pltpu.VMEM((16, 8, 128), F32),
        *ring_bufs(N1),
        pltpu.VMEM((2, 48, 128), F32),
        pltpu.VMEM((2, 48, 128), F32),
        pltpu.VMEM((768, 256), BF),
        pltpu.VMEM((8, 96, 256), BF),
        pltpu.VMEM((8, 96, 256), BF),
        pltpu.VMEM((768, 256), BF),
        pltpu.VMEM((768, 256), BF),
        pltpu.VMEM((16, 8, 128), F32),
        pltpu.VMEM((16, 8, 128), F32),
        pltpu.VMEM((768, 128), F32),
        *ring_bufs(N2),
        pltpu.VMEM((768, FFD), BF),
        pltpu.VMEM((256, 768), BF),
        pltpu.VMEM((8, 32, 768), BF),
        dma((14,)),
        dma((8,)), dma((8,)),
        dma((16,)), dma((16,)),
        dma((16,)), dma((16,)),
        dma((8,)), dma((8,)),
        dma((8,)), dma((8,)),
        dma((16,)), dma((16,)),
        dma((12,)), dma((12,)),
        dma((12,)), dma((12,)),
        dma((16,)), dma((16,)),
        dma((8,)), dma((8,)),
    ]
    specs = [any_spec] * 19
    for i in (1, 8, 10, 17, 18):
        specs[i] = vm_spec
    return pl.pallas_call(
        layer,
        out_shape=jax.ShapeDtypeStruct((768, 32), BF),
        in_specs=specs,
        out_specs=vm_spec,
        scratch_shapes=scratch,
        compiler_params=pltpu.CompilerParams(
            collective_id=0, has_side_effects=True, vmem_limit_bytes=60 * 1024 * 1024
        ),
    )(
        tokens, norm_gain.reshape(1, 256), w_query, w_key, w_value, w_outgate, w_igate, w_fgate,
        head_gain.reshape(1, 256), w_proj, mixer_gain.reshape(1, 256), w_gate, w_up, w_down,
        state_c, tail_keys, tail_values, tail_gate.reshape(48, 128), meta,
    )


def solution(mesh):
    kvtp = P("kv", "tp")
    return jax.shard_map(
        per_device,
        mesh=mesh,
        in_specs=(
            P(None, ("kv", "tp")), P("kv"), kvtp, kvtp, kvtp, kvtp, P(), P(), P("tp"), P("tp"),
            P("tp", "kv"), P("kv"), kvtp, kvtp, P("tp", "kv"), P("kv", "tp", None, None), kvtp,
            P("kv", "tp", None, None), P("kv", "tp", None, None), P("kv", "tp", None), kvtp, P("kv"),
        ),
        out_specs=P(None, ("kv", "tp")),
        check_vma=False,
    )
```

```python
import jax
import jax.numpy as jnp
from jax import lax
from jax.experimental import pallas as pl
from jax.experimental.pallas import tpu as pltpu
from jax.sharding import PartitionSpec as P

D = 4096
EPS = 1e-06
F32 = jnp.float32
BF = jnp.bfloat16
MESH = pl.DeviceIdType.MESH
N1 = 1024
N2 = 2816
FFD = 1408


def remote(src, dst, ss, rs, dev):
    return pltpu.make_async_remote_copy(
        src_ref=src, dst_ref=dst, send_sem=ss, recv_sem=rs, device_id=dev, device_id_type=MESH
    )


def mod4(v):
    return lax.rem(v, 4)


def transpose_padded(rows):
    missing = 128 - rows.shape[0]
    if missing:
        rows = jnp.concatenate([rows, jnp.zeros((missing, rows.shape[1]), F32)], axis=0)
    return rows.T


def column_of(row):
    return jnp.broadcast_to(row, (128, 128)).T


def layer(
    tokens, norm_gain, w_query, w_key, w_value, w_outgate, w_igate, w_fgate, head_gain, w_proj,
    mixer_gain, w_gate, w_up, w_down, state_c, tail_keys, tail_values, tail_gate, state_m, block_forget,
    lengths, forget_bias,
    out,
    wide_t, wide, scaled, wqkvo, wig_v, wfg_v, wproj_v, wgu, wdown_v, cbuf, kbuf, vbuf,
    gsend, grecv, rows_v, tg_v,
    a_p, a_own, a_in, a_comb, a_l, a_r, a_q, a_qin, a_qcomb, a_ql, a_qr,
    qs, mix_all, att_send, att_recv, mid_all, ssend, srecv, mid_sel,
    lhs4, sm_own, b_own, b_q, b_qin, b_qcomb, b_ql, b_qr,
    hid, fsend, frecv,
    lsem, tok_s, tok_r, g_s, g_r, mix_s, mix_r, att_s, att_r, mid_s, mid_r, sq_s, sq_r,
    ra_s, ra_r, rb_s, rb_r, ws_s, ws_r, sm_s, sm_r, h_s, h_r, f_s, f_r,
):
    kv = lax.axis_index("kv")
    tp = lax.axis_index("tp")
    z = lax.div(kv, 4)
    x = lax.rem(kv, 4)
    c = lax.rem(tp, 2)
    y = lax.div(tp, 2)
    pa = x * (1 - c) + z * c
    pb = z * (1 - c) + x * c

    def kv_of(ia, ib):
        return ia * (1 + 3 * c) + ib * (4 - 3 * c)

    def at_a(g):
        return (kv_of(mod4(pa + g), pb), tp)

    def at_b(g):
        return (kv_of(pa, mod4(pb + g)), tp)

    def kv_peer(i):
        return mod4(z + i // 4) * 4 + mod4(x + i % 4)

    def kv_from(i):
        return mod4(z + 4 - i // 4) * 4 + mod4(x + 4 - i % 4)

    def tp_peer(r):
        return lax.rem(tp + r, 8)

    def tp_from(r):
        return lax.rem(tp + 8 - r, 8)

    def rows48(k):
        return pl.ds(pl.multiple_of(k * 48, 16), 48)

    def rows96(k):
        return pl.ds(pl.multiple_of(k * 96, 32), 96)

    def rows32(k):
        return pl.ds(pl.multiple_of(k * 32, 32), 32)

    sends = []

    def send(*args):
        copy = remote(*args)
        copy.start()
        sends.append(copy)

    loads = [
        pltpu.make_async_copy(tokens, wide_t.at[rows32(tp)], lsem.at[0]),
        pltpu.make_async_copy(w_query, wqkvo.at[:, pl.ds(0, 256)], lsem.at[1]),
        pltpu.make_async_copy(w_key, wqkvo.at[:, pl.ds(256, 256)], lsem.at[2]),
        pltpu.make_async_copy(w_value, wqkvo.at[:, pl.ds(512, 256)], lsem.at[3]),
        pltpu.make_async_copy(w_outgate, wqkvo.at[:, pl.ds(768, 256)], lsem.at[4]),
        pltpu.make_async_copy(w_igate.at[:, pl.ds(pl.multiple_of(kv * 256, 256), 256)], wig_v, lsem.at[5]),
        pltpu.make_async_copy(w_fgate.at[:, pl.ds(pl.multiple_of(kv * 256, 256), 256)], wfg_v, lsem.at[6]),
        pltpu.make_async_copy(state_c, cbuf, lsem.at[7]),
        pltpu.make_async_copy(tail_keys, kbuf, lsem.at[8]),
        pltpu.make_async_copy(tail_values, vbuf, lsem.at[9]),
        pltpu.make_async_copy(w_proj, wproj_v, lsem.at[10]),
        pltpu.make_async_copy(w_gate, wgu.at[pl.ds(0, 256), pl.ds(0, FFD)], lsem.at[11]),
        pltpu.make_async_copy(w_up, wgu.at[pl.ds(0, 256), pl.ds(FFD, FFD)], lsem.at[12]),
        pltpu.make_async_copy(w_down, wdown_v, lsem.at[13]),
    ]
    for load in loads:
        load.start()

    barrier = pltpu.get_barrier_semaphore()
    for i in range(1, 16):
        pl.semaphore_signal(barrier, inc=1, device_id=(kv_peer(i), tp), device_id_type=MESH)
    for r in range(1, 8):
        pl.semaphore_signal(barrier, inc=1, device_id=(kv, tp_peer(r)), device_id_type=MESH)

    loads[0].wait()
    pl.semaphore_wait(barrier, 22)

    for r in range(1, 8):
        mine = wide_t.at[rows32(tp)]
        send(mine, mine, tok_s.at[r], tok_r.at[r], (kv, tp_peer(r)))

    early, late = (0, 96), (96, 160)

    def weight_rows(slot, part):
        return wgu.at[pl.ds(256 * slot + part[0], part[1])]

    def weight_send(src_slot, dst_slot, part, i, dev):
        send(weight_rows(src_slot, part), weight_rows(dst_slot, part), ws_s.at[i], ws_r.at[i], dev)

    def weight_wait(slot, part, i):
        dst = weight_rows(slot, part)
        remote(dst, dst, ws_s.at[i], ws_r.at[i], (kv, tp)).wait_recv()

    loads[11].wait()
    loads[12].wait()
    weight_send(0, 1, early, 0, at_a(1))
    weight_send(0, 3, early, 1, at_a(3))
    lane = lax.broadcasted_iota(jnp.int32, (128, 128), 1)
    for i in range(5, 7):
        loads[i].wait()
    grow = lax.broadcasted_iota(jnp.int32, (128, 16), 0)
    gcol = lax.broadcasted_iota(jnp.int32, (128, 16), 1)
    pick_i = jnp.where((grow < 2) & (gcol == 2 * tp + grow), 1.0, 0.0).astype(BF)
    pick_f = jnp.where((grow >= 2) & (grow < 4) & (gcol == 2 * tp + grow - 2), 1.0, 0.0).astype(BF)
    gate_w = (
        jnp.dot(pick_i, wig_v[...], preferred_element_type=F32)
        + jnp.dot(pick_f, wfg_v[...], preferred_element_type=F32)
    ).T.astype(BF)
    rows_v[...] = jnp.zeros((8, 128), F32)
    rows_v[0:2, 0:48] = block_forget[...]
    rows_v[2:4, 0:48] = state_m[...]
    rows_v[4:5, 0:48] = lengths[...].astype(F32)
    lane8 = lax.broadcasted_iota(jnp.int32, (8, 128), 1)

    def pair_row(first, second):
        a8 = jnp.broadcast_to(first, (8, 128))
        b8 = jnp.broadcast_to(second, (8, 128))
        return jnp.where(lane8 < 64, a8, pltpu.roll(b8, 64, 1))

    forget_row = pair_row(rows_v[0:1, :], rows_v[1:2, :])
    state_row = pair_row(rows_v[2:3, :], rows_v[3:4, :])
    length_row = pair_row(rows_v[4:5, :], rows_v[4:5, :])[0:1]
    bias_row = jnp.where(lane8 < 64, forget_bias[0], forget_bias[1])
    tg_v[...] = jnp.zeros((128, 128), F32)
    tg_v[0:48, 0:64] = tail_gate[:, 0, :]
    tg_v[64:112, 0:64] = tail_gate[:, 1, :]
    gate_t = tg_v[...].T[:64]
    lane64 = lax.broadcasted_iota(jnp.int32, (64, 128), 1)

    for r in range(1, 8):
        src = wide_t.at[rows32(tp_from(r))]
        remote(src, src, tok_s.at[r], tok_r.at[r], (kv, tp)).wait_recv()
    for b in range(6):
        block = wide_t[:, 128 * b : 128 * b + 128].astype(F32).T
        wide[128 * b : 128 * b + 128, :] = block.astype(BF)
        scaled[128 * b : 128 * b + 128, :] = (block * norm_gain[...]).astype(BF)

    def ring_sum(lhs, weights, n, tile, p, own, inn, comb, from_l, from_r, q, qin, qcomb, ql, qr, ss, rs, between):
        half = n // 2
        first, second = pl.ds(0, half), pl.ds(half, half)

        def group(g, put):
            ia = mod4(pa + g)
            rows = jnp.concatenate([lhs[rows48(kv_of(ia, ib)), :] for ib in range(4)], axis=0)

            def step(t, _):
                cols = pl.ds(pl.multiple_of(t * tile, tile), tile)
                put(cols, jnp.dot(rows, weights[:, cols], preferred_element_type=F32))
                return 0

            lax.fori_loop(0, n // tile, step, 0)

        def into(ref):
            def put(cols, value):
                ref[:, cols] = value.astype(ref.dtype)

            return put

        def add_rows(count, fn):
            def step(i, _):
                fn(pl.ds(pl.multiple_of(i * 16, 16), 16))
                return 0

            lax.fori_loop(0, count // 16, step, 0)

        def waited(dst, i):
            remote(dst, dst, ss.at[i], rs.at[i], (kv, tp)).wait_recv()

        right, left = at_a(1), at_a(3)
        group(2, into(p.at[0]))
        send(p.at[0, :, first], inn.at[0], ss.at[0], rs.at[0], right)
        send(p.at[0, :, second], inn.at[1], ss.at[1], rs.at[1], left)
        group(1, into(p.at[1]))
        send(p.at[1, :, second], from_l.at[:, second], ss.at[2], rs.at[2], right)
        group(3, into(p.at[2]))
        send(p.at[2, :, first], from_r.at[:, first], ss.at[3], rs.at[3], left)
        between()
        waited(inn.at[0], 0)

        def comb0(rows):
            comb[0, rows, :] = (p[1, rows, first].astype(F32) + inn[0, rows, :].astype(F32)).astype(BF)

        add_rows(192, comb0)
        send(comb.at[0], from_l.at[:, first], ss.at[4], rs.at[4], right)
        waited(inn.at[1], 1)

        def comb1(rows):
            comb[1, rows, :] = (p[2, rows, second].astype(F32) + inn[1, rows, :].astype(F32)).astype(BF)

        add_rows(192, comb1)
        send(comb.at[1], from_r.at[:, second], ss.at[5], rs.at[5], left)
        group(0, into(own))
        waited(from_l.at[:, second], 2)
        waited(from_r.at[:, first], 3)
        waited(from_l.at[:, first], 4)
        waited(from_r.at[:, second], 5)

        right, left = at_b(1), at_b(3)

        def total(g, put):
            base = mod4(pb + g) * 48
            for i in range(3):
                rows = pl.ds(pl.multiple_of(base + 16 * i, 16), 16)
                put(
                    pl.ds(16 * i, 16),
                    own[rows, :] + from_l[rows, :].astype(F32) + from_r[rows, :].astype(F32),
                )

        def into_q(j):
            def put(rows, value):
                q[j, rows, :] = value.astype(BF)

            return put

        total(2, into_q(0))
        send(q.at[0, :, first], qin.at[0], ss.at[6], rs.at[6], right)
        send(q.at[0, :, second], qin.at[1], ss.at[7], rs.at[7], left)
        total(1, into_q(1))
        send(q.at[1, :, second], ql.at[:, second], ss.at[8], rs.at[8], right)
        total(3, into_q(2))
        send(q.at[2, :, first], qr.at[:, first], ss.at[9], rs.at[9], left)
        waited(qin.at[0], 6)
        qcomb[0] = (q[1, :, first].astype(F32) + qin[0].astype(F32)).astype(BF)
        send(qcomb.at[0], ql.at[:, first], ss.at[10], rs.at[10], right)
        waited(qin.at[1], 7)
        qcomb[1] = (q[2, :, second].astype(F32) + qin[1].astype(F32)).astype(BF)
        send(qcomb.at[1], qr.at[:, second], ss.at[11], rs.at[11], left)
        mine = pl.ds(pl.multiple_of(pb * 48, 16), 48)
        waited(ql.at[:, second], 8)
        waited(qr.at[:, first], 9)
        waited(ql.at[:, first], 10)
        waited(qr.at[:, second], 11)

        def result(cols):
            return (
                own[mine, cols]
                + from_l[mine, cols].astype(F32)
                + from_r[mine, cols].astype(F32)
                + ql[:, cols].astype(F32)
                + qr[:, cols].astype(F32)
            )

        return result

    def small_sum(recv_ref, own_tile, ss, rs):
        acc = own_tile
        for i in range(1, 16):
            remote(recv_ref.at[i], recv_ref.at[i], ss.at[i], rs.at[i], (kv, tp)).wait_recv()
            acc = acc + recv_ref[i]
        return acc

    lane48 = lax.broadcasted_iota(jnp.int32, (48, 128), 1)

    def gate_tiles():
        def step(k, _):
            rows = rows48(k)
            part = jnp.dot(scaled[rows, :], gate_w, preferred_element_type=F32)
            wf = wide[rows, :].astype(F32)
            sq = jnp.sum(wf * wf, axis=1, keepdims=True)
            gsend[k] = transpose_padded(jnp.where(lane48 == 4, sq, part))[:8]
            return 0

        lax.fori_loop(0, 16, step, 0)
        for i in range(1, 16):
            k = kv_peer(i)
            send(gsend.at[k], grecv.at[i], g_s.at[i], g_r.at[i], (k, tp))

    for i in range(1, 5):
        loads[i].wait()
    proj = ring_sum(
        scaled, wqkvo, N1, 256, a_p, a_own, a_in, a_comb, a_l, a_r, a_q, a_qin, a_qcomb, a_ql, a_qr,
        ra_s, ra_r, gate_tiles,
    )
    weight_send(0, 1, late, 2, at_a(1))
    weight_send(0, 3, late, 3, at_a(3))
    gsum = small_sum(grecv, gsend[kv], g_s, g_r)
    inv_row = lax.rsqrt(gsum[4:5, :] / D + EPS)
    inv_col = column_of(inv_row)[:48]
    igate = pair_row(gsum[0:1, :] * inv_row, gsum[1:2, :] * inv_row)
    fpre = pair_row(gsum[2:3, :] * inv_row, gsum[3:4, :] * inv_row) + bias_row
    log_sig = -(jnp.maximum(-fpre, 0.0) + jnp.log1p(jnp.exp(-jnp.abs(fpre))))
    running = forget_row + log_sig
    inter = running + state_row
    pos = lax.broadcasted_iota(jnp.int32, (64, 128), 0).astype(F32)
    tail_log = jnp.where(pos < length_row, running[0:1] + gate_t, -jnp.inf)
    top = jnp.maximum(jnp.maximum(inter[0:1], jnp.max(tail_log, axis=0, keepdims=True)), igate[0:1])
    w_inter = jnp.exp(inter[0:1] - top)
    w_own = column_of(jnp.exp(igate[0:1] - top))
    w_tail = jnp.exp(tail_log - top)

    for h in range(2):
        qs[h] = proj(pl.ds(128 * h, 128)) * inv_col
    for i in range(7, 10):
        loads[i].wait()

    pad16 = jnp.zeros((16, 128), F32)
    q_t = jnp.concatenate([qs[0], pad16, qs[1], pad16], axis=0).T
    q_hi = q_t.astype(BF)
    q_lo = (q_t - q_hi.astype(F32)).astype(BF)
    q_cols = jnp.concatenate([q_hi, q_lo], axis=1)
    q_both = jnp.concatenate([q_cols, jnp.concatenate([q_hi, jnp.zeros((128, 128), BF)], axis=1)], axis=0)

    def recall_step(s, carry):
        mem_t, sc_t = carry
        for h in range(2):
            state = cbuf[s, h]
            s_hi = state.astype(BF)
            s_lo = (state - s_hi.astype(F32)).astype(BF)
            m = jnp.dot(jnp.concatenate([s_hi, s_lo], axis=1), q_both, preferred_element_type=F32)
            mem_t = jnp.where(lane == 64 * h + s, m[:, :128] + m[:, 128:], mem_t)
            sc = jnp.dot(kbuf[s, h], q_cols, preferred_element_type=F32)
            sc_t = jnp.where(lane64 == 64 * h + s, sc[:, :128] + sc[:, 128:], sc_t)
        return mem_t, sc_t

    mem_t, sc_t = lax.fori_loop(
        0, 48, recall_step, (jnp.zeros((128, 128), F32), jnp.zeros((64, 128), F32)), unroll=2
    )
    weighted = w_tail * (sc_t * 128 ** (-0.5))
    rows_w = jnp.concatenate([weighted, weighted], axis=0).T
    prow = lax.broadcasted_iota(jnp.int32, (128, 256), 0)
    plane = lax.broadcasted_iota(jnp.int32, (128, 256), 1)
    slot = 2 * lax.rem(prow, 2) + lax.div(prow, 64)
    rows_w = jnp.where(lax.div(plane, 64) == slot, jnp.concatenate([rows_w, rows_w], axis=1), 0.0)
    w_hi = rows_w.astype(BF)
    w_lo = (rows_w - w_hi.astype(F32)).astype(BF)
    step_of = lax.div(lax.rem(prow, 64), 2)

    def tail_step(g, acc):
        here = jnp.where(step_of == g, 1.0, 0.0).astype(BF)
        vals = vbuf[pl.ds(2 * g, 2)].reshape(256, 128)
        return (
            acc
            + jnp.dot(w_hi * here, vals, preferred_element_type=F32)
            + jnp.dot(w_lo * here, vals, preferred_element_type=F32)
        )

    tail_part = lax.fori_loop(0, 24, tail_step, jnp.zeros((128, 128), F32), unroll=2)
    memory = (mem_t * w_inter).T + tail_part
    mixed = []
    for h in range(2):
        q = qs[h]
        k = proj(pl.ds(256 + 128 * h, 128)) * inv_col * 128 ** (-0.5)
        v = proj(pl.ds(512 + 128 * h, 128)) * inv_col
        og = proj(pl.ds(768 + 128 * h, 128)) * inv_col
        own = jnp.sum(q * k, axis=1, keepdims=True)
        recalled = memory[64 * h : 64 * h + 48] + w_own[64 * h : 64 * h + 48] * own * v
        ms = jnp.mean(recalled * recalled, axis=1, keepdims=True)
        normed = recalled * lax.rsqrt(ms + EPS)
        hg = head_gain[:, 128 * h : 128 * h + 128]
        mixed.append((normed * hg * (1.0 / (1.0 + jnp.exp(-og)))).astype(BF))
    mix_all[rows48(kv), :] = jnp.concatenate(mixed, axis=1)
    for i in range(1, 16):
        mine = mix_all.at[rows48(kv)]
        send(mine, mine, mix_s.at[i], mix_r.at[i], (kv_peer(i), tp))
    loads[10].wait()
    for i in range(1, 16):
        src = mix_all.at[rows48(kv_from(i))]
        remote(src, src, mix_s.at[i], mix_r.at[i], (kv, tp)).wait_recv()

    for r in [4, 3, 5, 2, 6, 1, 7, 0]:
        part = jnp.dot(mix_all[rows96(tp_peer(r)), :], wproj_v[...], preferred_element_type=F32)
        att_send[r] = part.astype(BF)
        if r:
            send(att_send.at[r], att_recv.at[r], att_s.at[r], att_r.at[r], (kv, tp_peer(r)))
    weight_wait(1, early, 0)
    weight_wait(1, late, 2)
    weight_send(1, 2, (0, 128), 4, at_a(1))
    weight_wait(3, early, 1)
    weight_wait(3, late, 3)
    weight_send(3, 2, (128, 128), 5, at_a(3))
    attended = att_send[0].astype(F32)
    for r in range(1, 8):
        remote(att_recv.at[r], att_recv.at[r], att_s.at[r], att_r.at[r], (kv, tp)).wait_recv()
        attended = attended + att_recv[r].astype(F32)
    middle = (wide[rows96(tp), :].astype(F32) + attended).astype(BF)
    mid_all[rows96(tp), :] = middle
    middle_f = middle.astype(F32)
    sm_block = (middle_f * mixer_gain[...]).astype(BF)
    later = []

    def send_unless(here, *args):
        copy = remote(*args)

        @pl.when(jnp.logical_not(here))
        def _():
            copy.start()

        later.append((here, copy))

    for i in range(2):
        sm_own[i] = sm_block[48 * i : 48 * i + 48]
    for n, (dy, dc, i) in enumerate((dy, dc, i) for dy in (2, 1, 3, 0) for dc in range(2) for i in range(2)):
        k = 2 * tp + i
        kz, kx = lax.div(k, 4), lax.rem(k, 4)
        cd = lax.rem(c + dc, 2)
        dev_kv = (1 - cd) * (4 * z + kx) + cd * (4 * kz + x)
        ra = mod4((1 - cd) * (kx + 4 - x) + cd * (kz + 4 - z))
        ib = (1 - cd) * kz + cd * kx
        args = (
            sm_own.at[i], lhs4.at[ra, rows48(ib)], sm_s.at[n], sm_r.at[ra * 4 + ib],
            (dev_kv, 2 * mod4(y + dy) + cd),
        )
        if dy == 0 and dc == 0:
            send_unless(dev_kv == kv, *args)
        else:
            send(*args)
    for i in range(2):
        sq = middle_f[48 * i : 48 * i + 48]
        sq = sq * sq
        row = jnp.sum(transpose_padded(sq[:, :128] + sq[:, 128:]), axis=0, keepdims=True)
        ssend[i] = jnp.broadcast_to(row, (8, 128))
        k = 2 * tp + i
        slot = 4 * mod4(lax.div(k, 4) + 4 - z) + mod4(lax.rem(k, 4) + 4 - x)
        for r in range(8):
            args = (ssend.at[i], srecv.at[slot], sq_s.at[8 * i + r], sq_r.at[slot], (k, tp_peer(r)))
            if r == 0:
                send_unless(k == kv, *args)
            else:
                send(*args)
    for r in [4, 3, 5, 2, 6, 1, 7]:
        mine = mid_all.at[rows96(tp)]
        send(mine, mine, mid_s.at[r], mid_r.at[r], (kv, tp_peer(r)))

    for n in (4, 5):
        weight_wait(2, (128 * (n - 4), 128), n)
    for ra in range(4):
        for ib in range(4):
            dst = lhs4.at[ra, pl.ds(48 * ib, 48)]
            got = remote(dst, dst, sm_s.at[0], sm_r.at[ra * 4 + ib], (kv, tp))
            if ra:
                got.wait_recv()
            else:
                k = kv_of(pa, ib)
                here = lax.div(k, 2) == tp

                @pl.when(jnp.logical_not(here))
                def _():
                    got.wait_recv()

                @pl.when(here)
                def _():
                    lhs4[0, 48 * ib : 48 * ib + 48, :] = sm_own[lax.rem(k, 2)]
    rows_all = jnp.concatenate([lhs4[ra] for ra in range(4)], axis=1)
    first, second = pl.ds(0, FFD), pl.ds(FFD, FFD)

    def half_product(base):
        def step(t, _):
            cols = pl.ds(pl.multiple_of(base + t * 256, 128), 256)
            b_own[:, cols] = jnp.dot(rows_all, wgu[:, cols], preferred_element_type=F32)
            return 0

        lax.fori_loop(0, 5, step, 0)
        cols = pl.ds(base + 1280, 128)
        b_own[:, cols] = jnp.dot(rows_all, wgu[:, cols], preferred_element_type=F32)

    def b_rows(g):
        return pl.ds(pl.multiple_of(mod4(pb + g) * 48, 16), 48)

    def b_put(j, g, cols):
        b_q[j, :, cols] = b_own[b_rows(g), cols].astype(BF)

    def b_wait(dst, i):
        remote(dst, dst, rb_s.at[i], rb_r.at[i], (kv, tp)).wait_recv()

    right, left = at_b(1), at_b(3)
    half_product(0)
    b_put(0, 2, first)
    send(b_q.at[0, :, first], b_qin.at[0], rb_s.at[6], rb_r.at[6], right)
    b_put(2, 3, first)
    send(b_q.at[2, :, first], b_qr.at[:, first], rb_s.at[9], rb_r.at[9], left)
    half_product(FFD)
    b_put(0, 2, second)
    send(b_q.at[0, :, second], b_qin.at[1], rb_s.at[7], rb_r.at[7], left)
    b_put(1, 1, second)
    send(b_q.at[1, :, second], b_ql.at[:, second], rb_s.at[8], rb_r.at[8], right)
    b_wait(b_qin.at[0], 6)
    b_qcomb[0] = (b_own[b_rows(1), first] + b_qin[0].astype(F32)).astype(BF)
    send(b_qcomb.at[0], b_ql.at[:, first], rb_s.at[10], rb_r.at[10], right)
    b_wait(b_qin.at[1], 7)
    b_qcomb[1] = (b_own[b_rows(3), second] + b_qin[1].astype(F32)).astype(BF)
    send(b_qcomb.at[1], b_qr.at[:, second], rb_s.at[11], rb_r.at[11], left)
    for r in range(1, 8):
        src = mid_all.at[rows96(tp_from(r))]
        remote(src, src, mid_s.at[r], mid_r.at[r], (kv, tp)).wait_recv()
    srow = lax.broadcasted_iota(jnp.int32, (32, 256), 0)
    scol = lax.broadcasted_iota(jnp.int32, (32, 256), 1)
    pick = jnp.where(scol == 32 * tp + srow, 1.0, 0.0).astype(BF)
    mid_sel[...] = lax.dot_general(
        pick, mid_all[...], (((1,), (1,)), ((), ())), preferred_element_type=F32
    )
    sq_here = lax.div(kv, 2) == tp
    sq0 = remote(srecv.at[0], srecv.at[0], sq_s.at[0], sq_r.at[0], (kv, tp))

    @pl.when(jnp.logical_not(sq_here))
    def _():
        sq0.wait_recv()

    @pl.when(sq_here)
    def _():
        srecv[0] = ssend[lax.rem(kv, 2)]

    ssum = small_sum(srecv, srecv[0], sq_s, sq_r)
    inv_mid = column_of(lax.rsqrt(ssum[0:1] / D + EPS))[:48]
    b_wait(b_ql.at[:, second], 8)
    b_wait(b_qr.at[:, first], 9)
    b_wait(b_ql.at[:, first], 10)
    b_wait(b_qr.at[:, second], 11)

    def both(cols):
        return b_own[b_rows(0), cols] + b_ql[:, cols].astype(F32) + b_qr[:, cols].astype(F32)

    def hidden_step(t, _):
        cols = pl.ds(pl.multiple_of(t * 128, 128), 128)
        gate = both(cols) * inv_mid
        up = both(pl.ds(pl.multiple_of(t * 128 + FFD, 128), 128)) * inv_mid
        hid[rows48(kv), cols] = (gate * (1.0 / (1.0 + jnp.exp(-gate))) * up).astype(BF)
        return 0

    lax.fori_loop(0, FFD // 128, hidden_step, 0)

    part_rows = (pl.ds(0, 32), pl.ds(32, 16))

    def chunk(ra, rb):
        return hid.at[rows48(kv_of(mod4(pa + 4 - ra), mod4(pb + 4 - rb)))]

    def piece(ref, i):
        return ref.at[part_rows[i]]

    def hop(ref, i, dev):
        send(ref, ref, h_s.at[i], h_r.at[i], dev)

    def arrived(ref, i):
        remote(ref, ref, h_s.at[i], h_r.at[i], (kv, tp)).wait_recv()

    def spread(rb):
        hop(chunk(0, rb), 4 + rb, at_a(1))
        hop(chunk(0, rb), 8 + rb, at_a(3))

    hop(chunk(0, 0), 0, at_b(1))
    hop(chunk(0, 0), 1, at_b(3))
    spread(0)
    arrived(chunk(0, 1), 0)
    hop(piece(chunk(0, 1), 0), 2, at_b(1))
    spread(1)
    arrived(chunk(0, 3), 1)
    hop(piece(chunk(0, 3), 1), 3, at_b(3))
    spread(3)
    arrived(chunk(1, 0), 4)
    hop(chunk(1, 0), 12, at_a(1))
    arrived(piece(chunk(0, 2), 0), 2)
    arrived(piece(chunk(0, 2), 1), 3)
    spread(2)
    arrived(chunk(1, 1), 5)
    hop(chunk(1, 1), 13, at_a(1))
    arrived(chunk(3, 3), 11)
    hop(chunk(3, 3), 15, at_a(3))
    arrived(chunk(3, 2), 10)
    hop(chunk(3, 2), 14, at_a(3))
    loads[13].wait()
    arrived(chunk(1, 2), 6)
    arrived(chunk(1, 3), 7)
    arrived(chunk(3, 0), 8)
    arrived(chunk(3, 1), 9)
    for rb in range(4):
        arrived(chunk(2, rb), 12 + rb)

    for b in range(6):
        part = jnp.dot(hid[128 * b : 128 * b + 128, :], wdown_v[...], preferred_element_type=F32)
        fsend[:, 128 * b : 128 * b + 128] = part.T.astype(BF)
    for r in [4, 3, 5, 2, 6, 1, 7]:
        t = tp_peer(r)
        send(fsend.at[rows32(t)], frecv.at[r], f_s.at[r], f_r.at[r], (kv, t))
    total = fsend[rows32(tp), :].astype(F32)
    for r in range(1, 8):
        remote(frecv.at[r], frecv.at[r], f_s.at[r], f_r.at[r], (kv, tp)).wait_recv()
        total = total + frecv[r].astype(F32)
    out[...] = (mid_sel[...] + total).astype(BF)
    for copy in sends:
        copy.wait_send()
    for here, copy in later:
        @pl.when(jnp.logical_not(here))
        def _():
            copy.wait_send()


def per_device(
    tokens, norm_gain, w_query, w_key, w_value, w_outgate, w_igate, w_fgate, forget_bias, head_gain,
    w_proj, mixer_gain, w_gate, w_up, w_down, state_c, state_m, tail_keys, tail_values, tail_gate,
    block_forget, lengths,
):
    any_spec = pl.BlockSpec(memory_space=pl.ANY)
    vm_spec = pl.BlockSpec(memory_space=pltpu.VMEM)
    dma = pltpu.SemaphoreType.DMA

    def ring_bufs(n):
        return [
            pltpu.VMEM((3, 192, n), BF),
            pltpu.VMEM((192, n), F32),
            pltpu.VMEM((2, 192, n // 2), BF),
            pltpu.VMEM((2, 192, n // 2), BF),
            pltpu.VMEM((192, n), BF),
            pltpu.VMEM((192, n), BF),
            pltpu.VMEM((3, 48, n), BF),
            pltpu.VMEM((2, 48, n // 2), BF),
            pltpu.VMEM((2, 48, n // 2), BF),
            pltpu.VMEM((48, n), BF),
            pltpu.VMEM((48, n), BF),
        ]

    scratch = [
        pltpu.VMEM((256, 768), BF),
        pltpu.VMEM((768, 256), BF),
        pltpu.VMEM((768, 256), BF),
        pltpu.VMEM((256, N1), BF),
        pltpu.VMEM((16, 256), BF),
        pltpu.VMEM((16, 256), BF),
        pltpu.VMEM((256, 256), BF),
        pltpu.VMEM((1024, N2), BF),
        pltpu.VMEM((FFD, 256), BF),
        pltpu.VMEM((48, 2, 128, 128), F32),
        pltpu.VMEM((48, 2, 64, 128), BF),
        pltpu.VMEM((48, 2, 64, 128), BF),
        pltpu.VMEM((16, 8, 128), F32),
        pltpu.VMEM((16, 8, 128), F32),
        pltpu.VMEM((8, 128), F32),
        pltpu.VMEM((128, 128), F32),
        *ring_bufs(N1),
        pltpu.VMEM((2, 48, 128), F32),
        pltpu.VMEM((768, 256), BF),
        pltpu.VMEM((8, 96, 256), BF),
        pltpu.VMEM((8, 96, 256), BF),
        pltpu.VMEM((768, 256), BF),
        pltpu.VMEM((2, 8, 128), F32),
        pltpu.VMEM((16, 8, 128), F32),
        pltpu.VMEM((32, 768), F32),
        pltpu.VMEM((4, 192, 256), BF),
        pltpu.VMEM((2, 48, 256), BF),
        pltpu.VMEM((192, N2), F32),
        *ring_bufs(N2)[6:],
        pltpu.VMEM((768, FFD), BF),
        pltpu.VMEM((256, 768), BF),
        pltpu.VMEM((8, 32, 768), BF),
        dma((14,)),
        dma((8,)), dma((8,)),
        dma((16,)), dma((16,)),
        dma((16,)), dma((16,)),
        dma((8,)), dma((8,)),
        dma((8,)), dma((8,)),
        dma((16,)), dma((16,)),
        dma((12,)), dma((12,)),
        dma((12,)), dma((12,)),
        dma((6,)), dma((6,)),
        dma((16,)), dma((16,)),
        dma((16,)), dma((16,)),
        dma((8,)), dma((8,)),
    ]
    specs = [any_spec] * 21
    for i in (1, 8, 10, 17, 18, 19, 20):
        specs[i] = vm_spec
    specs.append(pl.BlockSpec(memory_space=pltpu.SMEM))
    result_t = pl.pallas_call(
        layer,
        out_shape=jax.ShapeDtypeStruct((32, 768), BF),
        in_specs=specs,
        out_specs=vm_spec,
        scratch_shapes=scratch,
        compiler_params=pltpu.CompilerParams(
            collective_id=0, has_side_effects=True, vmem_limit_bytes=60 * 1024 * 1024
        ),
    )(
        tokens.T, norm_gain.reshape(1, 256), w_query, w_key, w_value, w_outgate, w_igate.T, w_fgate.T,
        head_gain.reshape(1, 256), w_proj, mixer_gain.reshape(1, 256), w_gate, w_up, w_down,
        state_c, tail_keys, tail_values, tail_gate, state_m.T, block_forget.T, lengths.reshape(1, 48), forget_bias,
    )
    return result_t.T


def solution(mesh):
    kvtp = P("kv", "tp")
    return jax.shard_map(
        per_device,
        mesh=mesh,
        in_specs=(
            P(None, ("kv", "tp")), P("kv"), kvtp, kvtp, kvtp, kvtp, P(), P(), P("tp"), P("tp"),
            P("tp", "kv"), P("kv"), kvtp, kvtp, P("tp", "kv"), P("kv", "tp", None, None), kvtp,
            P("kv", "tp", None, None), P("kv", "tp", None, None), P("kv", "tp", None), kvtp, P("kv"),
        ),
        out_specs=P(None, ("kv", "tp")),
        check_vma=False,
    )
```

```python
import jax
import jax.numpy as jnp
from jax import lax
from jax.experimental import pallas as pl
from jax.experimental.pallas import tpu as pltpu
from jax.sharding import PartitionSpec as P

D = 4096
EPS = 1e-06
F32 = jnp.float32
BF = jnp.bfloat16
MESH = pl.DeviceIdType.MESH
N1 = 1024
N2 = 2816
FFD = 1408


def remote(src, dst, ss, rs, dev):
    return pltpu.make_async_remote_copy(
        src_ref=src, dst_ref=dst, send_sem=ss, recv_sem=rs, device_id=dev, device_id_type=MESH
    )


def mod4(v):
    return lax.rem(v, 4)


def transpose_padded(rows):
    missing = 128 - rows.shape[0]
    if missing:
        rows = jnp.concatenate([rows, jnp.zeros((missing, rows.shape[1]), F32)], axis=0)
    return rows.T


def column_of(row):
    return jnp.broadcast_to(row, (128, 128)).T


def layer(
    tokens, norm_gain, w_query, w_key, w_value, w_outgate, w_igate, w_fgate, head_gain, w_proj,
    mixer_gain, w_gate, w_up, w_down, state_c, tail_keys, tail_values, tail_gate, state_m, block_forget,
    lengths, forget_bias,
    out,
    wide_t, wide, scaled, wqkvo, wig_v, wfg_v, wproj_v, wgu, wdown_v, cbuf, kbuf, vbuf,
    gsend, grecv, rows_v, tg_v,
    a_p, a_own, a_in, a_comb, a_l, a_r, a_q, a_qin, a_qcomb, a_ql, a_qr,
    qs, q_rows, mem_n, sc_n, mix_all, att_send, att_recv, mid_all, ssend, srecv, mid_sel,
    lhs4, sm_own, b_own, b_q, b_qin, b_qcomb, b_ql, b_qr,
    hid, fsend, frecv, down_rows,
    lsem, tok_s, tok_r, g_s, g_r, mix_s, mix_r, att_s, att_r, mid_s, mid_r, sq_s, sq_r,
    ra_s, ra_r, rb_s, rb_r, ws_s, ws_r, sm_s, sm_r, wd_s, wd_r, h_s, h_r, f_s, f_r,
):
    kv = lax.axis_index("kv")
    tp = lax.axis_index("tp")
    z = lax.div(kv, 4)
    x = lax.rem(kv, 4)
    c = lax.rem(tp, 2)
    y = lax.div(tp, 2)
    pa = x * (1 - c) + z * c
    pb = z * (1 - c) + x * c

    def kv_of(ia, ib):
        return ia * (1 + 3 * c) + ib * (4 - 3 * c)

    def at_a(g):
        return (kv_of(mod4(pa + g), pb), tp)

    def at_b(g):
        return (kv_of(pa, mod4(pb + g)), tp)

    def kv_peer(i):
        return mod4(z + i // 4) * 4 + mod4(x + i % 4)

    def kv_from(i):
        return mod4(z + 4 - i // 4) * 4 + mod4(x + 4 - i % 4)

    def tp_peer(r):
        return lax.rem(tp + r, 8)

    def tp_from(r):
        return lax.rem(tp + 8 - r, 8)

    def rows48(k):
        return pl.ds(pl.multiple_of(k * 48, 16), 48)

    def rows96(k):
        return pl.ds(pl.multiple_of(k * 96, 32), 96)

    def rows32(k):
        return pl.ds(pl.multiple_of(k * 32, 32), 32)

    sends = []

    def send(*args):
        copy = remote(*args)
        copy.start()
        sends.append(copy)

    loads = [
        pltpu.make_async_copy(tokens, wide_t.at[rows32(tp)], lsem.at[0]),
        pltpu.make_async_copy(w_query, wqkvo.at[:, pl.ds(0, 256)], lsem.at[1]),
        pltpu.make_async_copy(w_key, wqkvo.at[:, pl.ds(256, 256)], lsem.at[2]),
        pltpu.make_async_copy(w_value, wqkvo.at[:, pl.ds(512, 256)], lsem.at[3]),
        pltpu.make_async_copy(w_outgate, wqkvo.at[:, pl.ds(768, 256)], lsem.at[4]),
        pltpu.make_async_copy(w_igate.at[:, pl.ds(pl.multiple_of(kv * 256, 256), 256)], wig_v, lsem.at[5]),
        pltpu.make_async_copy(w_fgate.at[:, pl.ds(pl.multiple_of(kv * 256, 256), 256)], wfg_v, lsem.at[6]),
        pltpu.make_async_copy(state_c, cbuf, lsem.at[7]),
        pltpu.make_async_copy(tail_keys, kbuf, lsem.at[8]),
        pltpu.make_async_copy(tail_values, vbuf, lsem.at[9]),
        pltpu.make_async_copy(w_proj, wproj_v, lsem.at[10]),
        pltpu.make_async_copy(w_gate, wgu.at[pl.ds(0, 256), pl.ds(0, FFD)], lsem.at[11]),
        pltpu.make_async_copy(w_up, wgu.at[pl.ds(0, 256), pl.ds(FFD, FFD)], lsem.at[12]),
        pltpu.make_async_copy(w_down, wdown_v.at[:, pl.ds(0, 256)], lsem.at[13]),
    ]
    for load in loads:
        load.start()

    barrier = pltpu.get_barrier_semaphore()
    for i in range(1, 16):
        pl.semaphore_signal(barrier, inc=1, device_id=(kv_peer(i), tp), device_id_type=MESH)
    for r in range(1, 8):
        pl.semaphore_signal(barrier, inc=1, device_id=(kv, tp_peer(r)), device_id_type=MESH)

    loads[0].wait()
    pl.semaphore_wait(barrier, 22)

    for r in range(1, 8):
        mine = wide_t.at[rows32(tp)]
        send(mine, mine, tok_s.at[r], tok_r.at[r], (kv, tp_peer(r)))

    early, late = (0, 96), (96, 160)

    def weight_rows(slot, part):
        return wgu.at[pl.ds(256 * slot + part[0], part[1])]

    def weight_send(src_slot, dst_slot, part, i, dev):
        send(weight_rows(src_slot, part), weight_rows(dst_slot, part), ws_s.at[i], ws_r.at[i], dev)

    def weight_wait(slot, part, i):
        dst = weight_rows(slot, part)
        remote(dst, dst, ws_s.at[i], ws_r.at[i], (kv, tp)).wait_recv()

    loads[11].wait()
    loads[12].wait()
    weight_send(0, 1, early, 0, at_a(1))
    weight_send(0, 3, early, 1, at_a(3))
    lane = lax.broadcasted_iota(jnp.int32, (128, 128), 1)
    for i in range(5, 7):
        loads[i].wait()
    grow = lax.broadcasted_iota(jnp.int32, (128, 16), 0)
    gcol = lax.broadcasted_iota(jnp.int32, (128, 16), 1)
    pick_i = jnp.where((grow < 2) & (gcol == 2 * tp + grow), 1.0, 0.0).astype(BF)
    pick_f = jnp.where((grow >= 2) & (grow < 4) & (gcol == 2 * tp + grow - 2), 1.0, 0.0).astype(BF)
    gate_w = (
        jnp.dot(pick_i, wig_v[...], preferred_element_type=F32)
        + jnp.dot(pick_f, wfg_v[...], preferred_element_type=F32)
    ).T.astype(BF)
    rows_v[...] = jnp.zeros((8, 128), F32)
    rows_v[0:2, 0:48] = block_forget[...]
    rows_v[2:4, 0:48] = state_m[...]
    rows_v[4:5, 0:48] = lengths[...].astype(F32)
    lane8 = lax.broadcasted_iota(jnp.int32, (8, 128), 1)

    def pair_row(first, second):
        a8 = jnp.broadcast_to(first, (8, 128))
        b8 = jnp.broadcast_to(second, (8, 128))
        return jnp.where(lane8 < 64, a8, pltpu.roll(b8, 64, 1))

    forget_row = pair_row(rows_v[0:1, :], rows_v[1:2, :])
    state_row = pair_row(rows_v[2:3, :], rows_v[3:4, :])
    length_row = pair_row(rows_v[4:5, :], rows_v[4:5, :])[0:1]
    bias_row = jnp.where(lane8 < 64, forget_bias[0], forget_bias[1])
    tg_v[...] = jnp.zeros((128, 128), F32)
    tg_v[0:48, 0:64] = tail_gate[:, 0, :]
    tg_v[64:112, 0:64] = tail_gate[:, 1, :]
    gate_t = tg_v[...].T[:64]
    lane64 = lax.broadcasted_iota(jnp.int32, (64, 128), 1)

    for r in range(1, 8):
        src = wide_t.at[rows32(tp_from(r))]
        remote(src, src, tok_s.at[r], tok_r.at[r], (kv, tp)).wait_recv()
    for b in range(6):
        block = wide_t[:, 128 * b : 128 * b + 128].astype(F32).T
        wide[128 * b : 128 * b + 128, :] = block.astype(BF)
        scaled[128 * b : 128 * b + 128, :] = (block * norm_gain[...]).astype(BF)

    def ring_sum(lhs, weights, n, tile, p, own, inn, comb, from_l, from_r, q, qin, qcomb, ql, qr, ss, rs, between):
        half = n // 2
        first, second = pl.ds(0, half), pl.ds(half, half)

        def group(g, put):
            ia = mod4(pa + g)
            rows = jnp.concatenate([lhs[rows48(kv_of(ia, ib)), :] for ib in range(4)], axis=0)

            def step(t, _):
                cols = pl.ds(pl.multiple_of(t * tile, tile), tile)
                put(cols, jnp.dot(rows, weights[:, cols], preferred_element_type=F32))
                return 0

            lax.fori_loop(0, n // tile, step, 0, unroll=True)

        def into(ref):
            def put(cols, value):
                ref[:, cols] = value.astype(ref.dtype)

            return put

        def add_rows(count, fn):
            def step(i, _):
                fn(pl.ds(pl.multiple_of(i * 16, 16), 16))
                return 0

            lax.fori_loop(0, count // 16, step, 0)

        def waited(dst, i):
            remote(dst, dst, ss.at[i], rs.at[i], (kv, tp)).wait_recv()

        right, left = at_a(1), at_a(3)
        group(2, into(p.at[0]))
        send(p.at[0, :, first], inn.at[0], ss.at[0], rs.at[0], right)
        send(p.at[0, :, second], inn.at[1], ss.at[1], rs.at[1], left)
        group(1, into(p.at[1]))
        send(p.at[1, :, second], from_l.at[:, second], ss.at[2], rs.at[2], right)
        group(3, into(p.at[2]))
        send(p.at[2, :, first], from_r.at[:, first], ss.at[3], rs.at[3], left)
        between()
        waited(inn.at[0], 0)

        def comb0(rows):
            comb[0, rows, :] = (p[1, rows, first].astype(F32) + inn[0, rows, :].astype(F32)).astype(BF)

        add_rows(192, comb0)
        send(comb.at[0], from_l.at[:, first], ss.at[4], rs.at[4], right)
        waited(inn.at[1], 1)

        def comb1(rows):
            comb[1, rows, :] = (p[2, rows, second].astype(F32) + inn[1, rows, :].astype(F32)).astype(BF)

        add_rows(192, comb1)
        send(comb.at[1], from_r.at[:, second], ss.at[5], rs.at[5], left)
        group(0, into(own))
        waited(from_l.at[:, second], 2)
        waited(from_r.at[:, first], 3)
        waited(from_l.at[:, first], 4)
        waited(from_r.at[:, second], 5)

        right, left = at_b(1), at_b(3)

        def total(g, put):
            base = mod4(pb + g) * 48
            for i in range(3):
                rows = pl.ds(pl.multiple_of(base + 16 * i, 16), 16)
                put(
                    pl.ds(16 * i, 16),
                    own[rows, :] + from_l[rows, :].astype(F32) + from_r[rows, :].astype(F32),
                )

        def into_q(j):
            def put(rows, value):
                q[j, rows, :] = value.astype(BF)

            return put

        total(2, into_q(0))
        send(q.at[0, :, first], qin.at[0], ss.at[6], rs.at[6], right)
        send(q.at[0, :, second], qin.at[1], ss.at[7], rs.at[7], left)
        weight_send(0, 1, late, 2, at_a(1))
        weight_send(0, 3, late, 3, at_a(3))
        total(1, into_q(1))
        send(q.at[1, :, second], ql.at[:, second], ss.at[8], rs.at[8], right)
        total(3, into_q(2))
        send(q.at[2, :, first], qr.at[:, first], ss.at[9], rs.at[9], left)
        waited(qin.at[0], 6)
        qcomb[0] = (q[1, :, first].astype(F32) + qin[0].astype(F32)).astype(BF)
        send(qcomb.at[0], ql.at[:, first], ss.at[10], rs.at[10], right)
        waited(qin.at[1], 7)
        qcomb[1] = (q[2, :, second].astype(F32) + qin[1].astype(F32)).astype(BF)
        send(qcomb.at[1], qr.at[:, second], ss.at[11], rs.at[11], left)
        mine = pl.ds(pl.multiple_of(pb * 48, 16), 48)
        waited(ql.at[:, second], 8)
        waited(qr.at[:, first], 9)
        waited(ql.at[:, first], 10)
        waited(qr.at[:, second], 11)

        def result(cols):
            return (
                own[mine, cols]
                + from_l[mine, cols].astype(F32)
                + from_r[mine, cols].astype(F32)
                + ql[:, cols].astype(F32)
                + qr[:, cols].astype(F32)
            )

        return result

    def small_sum(recv_ref, own_tile, ss, rs):
        acc = own_tile
        for i in range(1, 16):
            remote(recv_ref.at[i], recv_ref.at[i], ss.at[i], rs.at[i], (kv, tp)).wait_recv()
            acc = acc + recv_ref[i]
        return acc

    lane48 = lax.broadcasted_iota(jnp.int32, (48, 128), 1)

    def gate_tiles():
        def step(k, _):
            rows = rows48(k)
            part = jnp.dot(scaled[rows, :], gate_w, preferred_element_type=F32)
            wf = wide[rows, :].astype(F32)
            sq = jnp.sum(wf * wf, axis=1, keepdims=True)
            gsend[k] = transpose_padded(jnp.where(lane48 == 4, sq, part))[:8]
            return 0

        lax.fori_loop(0, 16, step, 0, unroll=4)
        for i in range(1, 16):
            k = kv_peer(i)
            send(gsend.at[k], grecv.at[i], g_s.at[i], g_r.at[i], (k, tp))

    for i in range(1, 5):
        loads[i].wait()
    proj = ring_sum(
        scaled, wqkvo, N1, 256, a_p, a_own, a_in, a_comb, a_l, a_r, a_q, a_qin, a_qcomb, a_ql, a_qr,
        ra_s, ra_r, gate_tiles,
    )
    gsum = small_sum(grecv, gsend[kv], g_s, g_r)
    inv_row = lax.rsqrt(gsum[4:5, :] / D + EPS)
    inv_col = column_of(inv_row)[:48]
    igate = pair_row(gsum[0:1, :] * inv_row, gsum[1:2, :] * inv_row)
    fpre = pair_row(gsum[2:3, :] * inv_row, gsum[3:4, :] * inv_row) + bias_row
    log_sig = -(jnp.maximum(-fpre, 0.0) + jnp.log1p(jnp.exp(-jnp.abs(fpre))))
    running = forget_row + log_sig
    inter = running + state_row
    pos = lax.broadcasted_iota(jnp.int32, (64, 128), 0).astype(F32)
    tail_log = jnp.where(pos < length_row, running[0:1] + gate_t, -jnp.inf)
    top = jnp.maximum(jnp.maximum(inter[0:1], jnp.max(tail_log, axis=0, keepdims=True)), igate[0:1])
    w_inter = jnp.exp(inter[0:1] - top)
    w_own = column_of(jnp.exp(igate[0:1] - top))
    w_tail = jnp.exp(tail_log - top)

    for h in range(2):
        qs[h] = proj(pl.ds(128 * h, 128)) * inv_col
    for i in range(7, 10):
        loads[i].wait()

    for h in range(2):
        q_hi = qs[h].astype(BF).astype(F32)
        q_lo = (qs[h] - q_hi).astype(BF).astype(F32)
        q_rows[:, 2 * h, :] = jnp.concatenate([q_hi, q_hi], axis=1)
        q_rows[:, 2 * h + 1, :] = jnp.concatenate([q_lo, jnp.zeros((48, 128), F32)], axis=1)
    for i in range(4, 8):
        q_rows[:, i, :] = jnp.zeros((48, 256), F32)
    contract_last = (((1,), (1,)), ((), ()))
    lane1 = lax.broadcasted_iota(jnp.int32, (1, 128), 1)

    def recall_step(s, _):
        lhs = q_rows[s].astype(BF)
        state = cbuf[s].reshape(256, 128)
        s_hi = state.astype(BF)
        s_lo = (state - s_hi.astype(F32)).astype(BF)
        m = lax.dot_general(
            lhs, jnp.concatenate([s_hi, s_lo], axis=1), contract_last, preferred_element_type=F32
        )
        mem_n[0, pl.ds(s, 1), :] = m[0:1, :128] + m[1:2, :128]
        mem_n[1, pl.ds(s, 1), :] = m[2:3, 128:] + m[3:4, 128:]
        sc = lax.dot_general(
            lhs[:, :128], kbuf[s].reshape(128, 128), contract_last, preferred_element_type=F32
        )
        sc_n[pl.ds(s, 1), :] = jnp.where(lane1 < 64, sc[0:1] + sc[1:2], sc[2:3] + sc[3:4])
        return 0

    lax.fori_loop(0, 48, recall_step, 0, unroll=4)
    sc_r = transpose_padded(sc_n[...])
    sc_t = jnp.where(lane64 < 64, sc_r[:64], pltpu.roll(sc_r[64:], 64, 1))
    weighted = w_tail * (sc_t * 128 ** (-0.5))
    rows_w = jnp.concatenate([weighted, weighted], axis=0).T
    prow = lax.broadcasted_iota(jnp.int32, (128, 256), 0)
    plane = lax.broadcasted_iota(jnp.int32, (128, 256), 1)
    slot = 2 * lax.rem(prow, 2) + lax.div(prow, 64)
    rows_w = jnp.where(lax.div(plane, 64) == slot, jnp.concatenate([rows_w, rows_w], axis=1), 0.0)
    w_hi = rows_w.astype(BF)
    w_lo = (rows_w - w_hi.astype(F32)).astype(BF)
    step_of = lax.div(lax.rem(prow, 64), 2)

    def tail_step(g, acc):
        here = jnp.where(step_of == g, 1.0, 0.0).astype(BF)
        vals = vbuf[pl.ds(2 * g, 2)].reshape(256, 128)
        return (
            acc
            + jnp.dot(w_hi * here, vals, preferred_element_type=F32)
            + jnp.dot(w_lo * here, vals, preferred_element_type=F32)
        )

    tail_part = lax.fori_loop(0, 24, tail_step, jnp.zeros((128, 128), F32), unroll=4)
    w_state = column_of(w_inter)
    mixed = []
    for h in range(2):
        q = qs[h]
        k = proj(pl.ds(256 + 128 * h, 128)) * inv_col * 128 ** (-0.5)
        v = proj(pl.ds(512 + 128 * h, 128)) * inv_col
        og = proj(pl.ds(768 + 128 * h, 128)) * inv_col
        own = jnp.sum(q * k, axis=1, keepdims=True)
        rows = slice(64 * h, 64 * h + 48)
        recalled = mem_n[h] * w_state[rows] + tail_part[rows] + w_own[rows] * own * v
        ms = jnp.mean(recalled * recalled, axis=1, keepdims=True)
        normed = recalled * lax.rsqrt(ms + EPS)
        hg = head_gain[:, 128 * h : 128 * h + 128]
        mixed.append((normed * hg * (1.0 / (1.0 + jnp.exp(-og)))).astype(BF))
    mix_all[rows48(kv), :] = jnp.concatenate(mixed, axis=1)
    for i in range(1, 16):
        mine = mix_all.at[rows48(kv)]
        send(mine, mine, mix_s.at[i], mix_r.at[i], (kv_peer(i), tp))
    loads[10].wait()
    for i in range(1, 16):
        src = mix_all.at[rows48(kv_from(i))]
        remote(src, src, mix_s.at[i], mix_r.at[i], (kv, tp)).wait_recv()

    weight_wait(1, early, 0)
    weight_wait(1, late, 2)
    weight_send(1, 2, (0, 128), 4, at_a(1))
    weight_wait(3, early, 1)
    weight_wait(3, late, 3)
    weight_send(3, 2, (128, 128), 5, at_a(3))
    for r in [4, 3, 5, 2, 6, 1, 7, 0]:
        part = jnp.dot(mix_all[rows96(tp_peer(r)), :], wproj_v[...], preferred_element_type=F32)
        att_send[r] = part.astype(BF)
        if r:
            send(att_send.at[r], att_recv.at[r], att_s.at[r], att_r.at[r], (kv, tp_peer(r)))
    attended = att_send[0].astype(F32)
    for r in range(1, 8):
        remote(att_recv.at[r], att_recv.at[r], att_s.at[r], att_r.at[r], (kv, tp)).wait_recv()
        attended = attended + att_recv[r].astype(F32)
    middle = (wide[rows96(tp), :].astype(F32) + attended).astype(BF)
    mid_all[rows96(tp), :] = middle
    middle_f = middle.astype(F32)
    sm_block = (middle_f * mixer_gain[...]).astype(BF)
    later = []

    def send_unless(here, *args):
        copy = remote(*args)

        @pl.when(jnp.logical_not(here))
        def _():
            copy.start()

        later.append((here, copy))

    for i in range(2):
        sm_own[i] = sm_block[48 * i : 48 * i + 48]
    for n, (dy, dc, i) in enumerate((dy, dc, i) for dy in (2, 1, 3, 0) for dc in range(2) for i in range(2)):
        k = 2 * tp + i
        kz, kx = lax.div(k, 4), lax.rem(k, 4)
        cd = lax.rem(c + dc, 2)
        dev_kv = (1 - cd) * (4 * z + kx) + cd * (4 * kz + x)
        ra = mod4((1 - cd) * (kx + 4 - x) + cd * (kz + 4 - z))
        ib = (1 - cd) * kz + cd * kx
        args = (
            sm_own.at[i], lhs4.at[ra, rows48(ib)], sm_s.at[n], sm_r.at[ra * 4 + ib],
            (dev_kv, 2 * mod4(y + dy) + cd),
        )
        if dy == 0 and dc == 0:
            send_unless(dev_kv == kv, *args)
        else:
            send(*args)
    for i in range(2):
        sq = middle_f[48 * i : 48 * i + 48]
        sq = sq * sq
        row = jnp.sum(transpose_padded(sq[:, :128] + sq[:, 128:]), axis=0, keepdims=True)
        ssend[i] = jnp.broadcast_to(row, (8, 128))
        k = 2 * tp + i
        slot = 4 * mod4(lax.div(k, 4) + 4 - z) + mod4(lax.rem(k, 4) + 4 - x)
        for r in range(8):
            args = (ssend.at[i], srecv.at[slot], sq_s.at[8 * i + r], sq_r.at[slot], (k, tp_peer(r)))
            if r == 0:
                send_unless(k == kv, *args)
            else:
                send(*args)
    def down_weights(slot, part=(0, FFD)):
        return wdown_v.at[pl.ds(part[0], part[1]), pl.ds(256 * slot, 256)]

    def down_send(src_slot, dst_slot, part, i, dev):
        send(down_weights(src_slot, part), down_weights(dst_slot, part), wd_s.at[i], wd_r.at[i], dev)

    def down_got(slot, part, i):
        dst = down_weights(slot, part)
        remote(dst, dst, wd_s.at[i], wd_r.at[i], (kv, tp)).wait_recv()

    whole, upper, lower = (0, FFD), (0, FFD // 2), (FFD // 2, FFD // 2)
    loads[13].wait()
    down_send(0, 1, whole, 0, at_a(1))
    down_send(0, 3, whole, 1, at_a(3))
    for r in [4, 3, 5, 2, 6, 1, 7]:
        mine = mid_all.at[rows96(tp)]
        send(mine, mine, mid_s.at[r], mid_r.at[r], (kv, tp_peer(r)))

    for n in (4, 5):
        weight_wait(2, (128 * (n - 4), 128), n)
    for ra in range(4):
        for ib in range(4):
            dst = lhs4.at[ra, pl.ds(48 * ib, 48)]
            got = remote(dst, dst, sm_s.at[0], sm_r.at[ra * 4 + ib], (kv, tp))
            if ra:
                got.wait_recv()
            else:
                k = kv_of(pa, ib)
                here = lax.div(k, 2) == tp

                @pl.when(jnp.logical_not(here))
                def _():
                    got.wait_recv()

                @pl.when(here)
                def _():
                    lhs4[0, 48 * ib : 48 * ib + 48, :] = sm_own[lax.rem(k, 2)]
    rows_all = jnp.concatenate([lhs4[ra] for ra in range(4)], axis=1)
    first, second = pl.ds(0, FFD), pl.ds(FFD, FFD)

    def half_product(base):
        def step(t, _):
            cols = pl.ds(pl.multiple_of(base + t * 256, 128), 256)
            b_own[:, cols] = jnp.dot(rows_all, wgu[:, cols], preferred_element_type=F32)
            return 0

        lax.fori_loop(0, 5, step, 0, unroll=True)
        cols = pl.ds(base + 1280, 128)
        b_own[:, cols] = jnp.dot(rows_all, wgu[:, cols], preferred_element_type=F32)

    def b_rows(g):
        return pl.ds(pl.multiple_of(mod4(pb + g) * 48, 16), 48)

    def b_put(j, g, cols):
        b_q[j, :, cols] = b_own[b_rows(g), cols].astype(BF)

    def b_wait(dst, i):
        remote(dst, dst, rb_s.at[i], rb_r.at[i], (kv, tp)).wait_recv()

    right, left = at_b(1), at_b(3)
    half_product(0)
    b_put(0, 2, first)
    send(b_q.at[0, :, first], b_qin.at[0], rb_s.at[6], rb_r.at[6], right)
    b_put(2, 3, first)
    send(b_q.at[2, :, first], b_qr.at[:, first], rb_s.at[9], rb_r.at[9], left)
    half_product(FFD)
    b_put(0, 2, second)
    send(b_q.at[0, :, second], b_qin.at[1], rb_s.at[7], rb_r.at[7], left)
    b_put(1, 1, second)
    send(b_q.at[1, :, second], b_ql.at[:, second], rb_s.at[8], rb_r.at[8], right)
    b_wait(b_qin.at[0], 6)
    b_qcomb[0] = (b_own[b_rows(1), first] + b_qin[0].astype(F32)).astype(BF)
    send(b_qcomb.at[0], b_ql.at[:, first], rb_s.at[10], rb_r.at[10], right)
    b_wait(b_qin.at[1], 7)
    b_qcomb[1] = (b_own[b_rows(3), second] + b_qin[1].astype(F32)).astype(BF)
    send(b_qcomb.at[1], b_qr.at[:, second], rb_s.at[11], rb_r.at[11], left)
    down_got(1, whole, 0)
    down_send(1, 2, upper, 2, at_a(1))
    down_got(3, whole, 1)
    down_send(3, 2, lower, 3, at_a(3))
    for r in range(1, 8):
        src = mid_all.at[rows96(tp_from(r))]
        remote(src, src, mid_s.at[r], mid_r.at[r], (kv, tp)).wait_recv()
    srow = lax.broadcasted_iota(jnp.int32, (32, 256), 0)
    scol = lax.broadcasted_iota(jnp.int32, (32, 256), 1)
    pick = jnp.where(scol == 32 * tp + srow, 1.0, 0.0).astype(BF)
    mid_sel[...] = lax.dot_general(
        pick, mid_all[...], (((1,), (1,)), ((), ())), preferred_element_type=F32
    )
    sq_here = lax.div(kv, 2) == tp
    sq0 = remote(srecv.at[0], srecv.at[0], sq_s.at[0], sq_r.at[0], (kv, tp))

    @pl.when(jnp.logical_not(sq_here))
    def _():
        sq0.wait_recv()

    @pl.when(sq_here)
    def _():
        srecv[0] = ssend[lax.rem(kv, 2)]

    ssum = small_sum(srecv, srecv[0], sq_s, sq_r)
    inv_mid = column_of(lax.rsqrt(ssum[0:1] / D + EPS))[:48]
    b_wait(b_ql.at[:, second], 8)
    b_wait(b_qr.at[:, first], 9)
    b_wait(b_ql.at[:, first], 10)
    b_wait(b_qr.at[:, second], 11)

    def both(cols):
        return b_own[b_rows(0), cols] + b_ql[:, cols].astype(F32) + b_qr[:, cols].astype(F32)

    def hidden_step(t, _):
        cols = pl.ds(pl.multiple_of(t * 128, 128), 128)
        gate = both(cols) * inv_mid
        up = both(pl.ds(pl.multiple_of(t * 128 + FFD, 128), 128)) * inv_mid
        hid[rows48(pb), cols] = (gate * (1.0 / (1.0 + jnp.exp(-gate))) * up).astype(BF)
        return 0

    lax.fori_loop(0, FFD // 128, hidden_step, 0)

    def chunk(rb, part=(0, 48)):
        return hid.at[pl.ds(pl.multiple_of(mod4(pb + 4 - rb) * 48 + part[0], 16), part[1])]

    def hop(ref, i, dev):
        send(ref, ref, h_s.at[i], h_r.at[i], dev)

    def arrived(ref, i):
        remote(ref, ref, h_s.at[i], h_r.at[i], (kv, tp)).wait_recv()

    hop(chunk(0), 0, at_b(1))
    hop(chunk(0), 1, at_b(3))
    arrived(chunk(1), 0)
    hop(chunk(1, (0, 32)), 2, at_b(1))
    arrived(chunk(3), 1)
    hop(chunk(3, (32, 16)), 3, at_b(3))
    down_got(2, upper, 2)
    down_got(2, lower, 3)
    arrived(chunk(2, (0, 32)), 2)
    arrived(chunk(2, (32, 16)), 3)

    lane16 = lax.broadcasted_iota(jnp.int32, (8, 16, 128), 2)
    for ra in (2, 1, 3, 0):
        part = jnp.dot(hid[...], wdown_v[:, 256 * ra : 256 * ra + 256], preferred_element_type=F32)
        part = jnp.concatenate([part, jnp.zeros((64, 256), F32)], axis=0).T
        tail = part[:, 128:].reshape(8, 2, 16, 128)
        tail = jnp.where(lane16 < 64, tail[:, 0], pltpu.roll(tail[:, 1], 64, 2))
        fsend[ra, :, 0:32, :] = part[:, :128].reshape(8, 32, 128).astype(BF)
        fsend[ra, :, 32:48, :] = tail.astype(BF)
        for dy in (2, 1, 3, 0):
            for dc in range(2):
                t = 2 * mod4(y + dy) + lax.rem(c + dc, 2)
                if ra or dy or dc:
                    send(
                        fsend.at[ra, t], frecv.at[c, ra, dy], f_s.at[8 * ra + 2 * dy + dc],
                        f_r.at[16 * c + 4 * ra + dy], (kv_of(mod4(pa + 4 - ra), pb), t),
                    )
    frecv[c, 0, 0] = fsend[0, tp]
    other = frecv.at[1 - c, 0, 0]
    remote(other, other, f_s.at[0], f_r.at[16 * (1 - c)], (kv, tp)).wait_recv()
    for cs in range(2):
        mains, tails = [], []
        for ra in range(4):
            piece = 0.0
            for dy in range(4):
                dst = frecv.at[cs, ra, dy]
                if ra or dy:
                    remote(dst, dst, f_s.at[0], f_r.at[16 * cs + 4 * ra + dy], (kv, tp)).wait_recv()
                piece = piece + frecv[cs, ra, dy].astype(F32)
            mains.append(piece[:32])
            tails += [piece[32:], pltpu.roll(piece[32:], 64, 1)]
        by_seq = jnp.concatenate(
            [jnp.concatenate(mains, axis=0).T, jnp.concatenate(tails, axis=0).T[:64]], axis=0
        )
        for ra in range(4):
            block = pltpu.roll(by_seq, (128 - 32 * ra) % 128, 1) if ra else by_seq
            for ib in range(4):
                k = 4 * ib + mod4(x + ra) if cs == 0 else 4 * mod4(z + ra) + ib
                mine = block[48 * ib : 48 * ib + 48]
                if cs == 0:
                    down_rows[rows48(k), :] = mine
                else:
                    down_rows[rows48(k), :] += mine
    for b in range(6):
        cols = slice(128 * b, 128 * b + 128)
        out[:, cols] = (mid_sel[:, cols] + down_rows[cols, :].T[:32]).astype(BF)
    for copy in sends:
        copy.wait_send()
    for here, copy in later:
        @pl.when(jnp.logical_not(here))
        def _():
            copy.wait_send()


def per_device(
    tokens, norm_gain, w_query, w_key, w_value, w_outgate, w_igate, w_fgate, forget_bias, head_gain,
    w_proj, mixer_gain, w_gate, w_up, w_down, state_c, state_m, tail_keys, tail_values, tail_gate,
    block_forget, lengths,
):
    any_spec = pl.BlockSpec(memory_space=pl.ANY)
    vm_spec = pl.BlockSpec(memory_space=pltpu.VMEM)
    dma = pltpu.SemaphoreType.DMA

    def ring_bufs(n):
        return [
            pltpu.VMEM((3, 192, n), BF),
            pltpu.VMEM((192, n), F32),
            pltpu.VMEM((2, 192, n // 2), BF),
            pltpu.VMEM((2, 192, n // 2), BF),
            pltpu.VMEM((192, n), BF),
            pltpu.VMEM((192, n), BF),
            pltpu.VMEM((3, 48, n), BF),
            pltpu.VMEM((2, 48, n // 2), BF),
            pltpu.VMEM((2, 48, n // 2), BF),
            pltpu.VMEM((48, n), BF),
            pltpu.VMEM((48, n), BF),
        ]

    scratch = [
        pltpu.VMEM((256, 768), BF),
        pltpu.VMEM((768, 256), BF),
        pltpu.VMEM((768, 256), BF),
        pltpu.VMEM((256, N1), BF),
        pltpu.VMEM((16, 256), BF),
        pltpu.VMEM((16, 256), BF),
        pltpu.VMEM((256, 256), BF),
        pltpu.VMEM((1024, N2), BF),
        pltpu.VMEM((FFD, 1024), BF),
        pltpu.VMEM((48, 2, 128, 128), F32),
        pltpu.VMEM((48, 2, 64, 128), BF),
        pltpu.VMEM((48, 2, 64, 128), BF),
        pltpu.VMEM((16, 8, 128), F32),
        pltpu.VMEM((16, 8, 128), F32),
        pltpu.VMEM((8, 128), F32),
        pltpu.VMEM((128, 128), F32),
        *ring_bufs(N1),
        pltpu.VMEM((2, 48, 128), F32),
        pltpu.VMEM((48, 8, 256), F32),
        pltpu.VMEM((2, 48, 128), F32),
        pltpu.VMEM((48, 128), F32),
        pltpu.VMEM((768, 256), BF),
        pltpu.VMEM((8, 96, 256), BF),
        pltpu.VMEM((8, 96, 256), BF),
        pltpu.VMEM((768, 256), BF),
        pltpu.VMEM((2, 8, 128), F32),
        pltpu.VMEM((16, 8, 128), F32),
        pltpu.VMEM((32, 768), F32),
        pltpu.VMEM((4, 192, 256), BF),
        pltpu.VMEM((2, 48, 256), BF),
        pltpu.VMEM((192, N2), F32),
        *ring_bufs(N2)[6:],
        pltpu.VMEM((192, FFD), BF),
        pltpu.VMEM((4, 8, 48, 128), BF),
        pltpu.VMEM((2, 4, 4, 48, 128), BF),
        pltpu.VMEM((768, 128), F32),
        dma((14,)),
        dma((8,)), dma((8,)),
        dma((16,)), dma((16,)),
        dma((16,)), dma((16,)),
        dma((8,)), dma((8,)),
        dma((8,)), dma((8,)),
        dma((16,)), dma((16,)),
        dma((12,)), dma((12,)),
        dma((12,)), dma((12,)),
        dma((6,)), dma((6,)),
        dma((16,)), dma((16,)),
        dma((4,)), dma((4,)),
        dma((4,)), dma((4,)),
        dma((32,)), dma((32,)),
    ]
    specs = [any_spec] * 21
    for i in (1, 8, 10, 17, 18, 19, 20):
        specs[i] = vm_spec
    specs.append(pl.BlockSpec(memory_space=pltpu.SMEM))
    result_t = pl.pallas_call(
        layer,
        out_shape=jax.ShapeDtypeStruct((32, 768), BF),
        in_specs=specs,
        out_specs=vm_spec,
        scratch_shapes=scratch,
        compiler_params=pltpu.CompilerParams(
            collective_id=0, has_side_effects=True, vmem_limit_bytes=60 * 1024 * 1024
        ),
    )(
        tokens.T, norm_gain.reshape(1, 256), w_query, w_key, w_value, w_outgate, w_igate.T, w_fgate.T,
        head_gain.reshape(1, 256), w_proj, mixer_gain.reshape(1, 256), w_gate, w_up, w_down,
        state_c, tail_keys, tail_values, tail_gate, state_m.T, block_forget.T, lengths.reshape(1, 48), forget_bias,
    )
    return result_t.T


def solution(mesh):
    kvtp = P("kv", "tp")
    return jax.shard_map(
        per_device,
        mesh=mesh,
        in_specs=(
            P(None, ("kv", "tp")), P("kv"), kvtp, kvtp, kvtp, kvtp, P(), P(), P("tp"), P("tp"),
            P("tp", "kv"), P("kv"), kvtp, kvtp, P("tp", "kv"), P("kv", "tp", None, None), kvtp,
            P("kv", "tp", None, None), P("kv", "tp", None, None), P("kv", "tp", None), kvtp, P("kv"),
        ),
        out_specs=P(None, ("kv", "tp")),
        check_vma=False,
    )
```

```python
import jax
import jax.numpy as jnp
from jax import lax
from jax.experimental import pallas as pl
from jax.experimental.pallas import tpu as pltpu
from jax.sharding import PartitionSpec as P

D = 4096
EPS = 1e-06
F32 = jnp.float32
BF = jnp.bfloat16
MESH = pl.DeviceIdType.MESH
N1 = 1024
NH = 512
N2 = 2816
FFD = 1408


def remote(src, dst, ss, rs, dev):
    return pltpu.make_async_remote_copy(
        src_ref=src, dst_ref=dst, send_sem=ss, recv_sem=rs, device_id=dev, device_id_type=MESH
    )


def mod4(v):
    return lax.rem(v, 4)


def transpose_padded(rows):
    missing = 128 - rows.shape[0]
    if missing:
        rows = jnp.concatenate([rows, jnp.zeros((missing, rows.shape[1]), F32)], axis=0)
    return rows.T


def column_of(row):
    return jnp.broadcast_to(row, (128, 128)).T


def layer(
    tokens, norm_gain, w_query, w_key, w_value, w_outgate, w_igate, w_fgate, head_gain, w_proj,
    mixer_gain, w_gate, w_up, w_down, state_c, tail_keys, tail_values, tail_gate, state_m, block_forget,
    lengths, forget_bias,
    out,
    wide_t, wide, scaled, wqkvo, wig_v, wfg_v, wproj_v, wgu, wdown_v, cbuf, kbuf, vbuf,
    gsend, grecv, rows_v, tg_v,
    *rest,
):
    qk_bufs, vo_bufs, rest = rest[:13], rest[13:26], rest[26:]
    (
        qs, q_rows, mem_n, sc_n, mix_all, att_send, att_recv, mid_all, ssend, srecv, mid_sel,
        lhs4, sm_own, b_own, b_q, b_qin, b_qcomb, b_ql, b_qr,
        hid, fsend, frecv, down_rows,
        lsem, tok_s, tok_r, g_s, g_r, mix_s, mix_r, att_s, att_r, mid_s, mid_r, sq_s, sq_r,
        qk_s, qk_r, vo_s, vo_r, rb_s, rb_r, ws_s, ws_r, sm_s, sm_r, wd_s, wd_r, h_s, h_r, f_s, f_r,
    ) = rest
    kv = lax.axis_index("kv")
    tp = lax.axis_index("tp")
    z = lax.div(kv, 4)
    x = lax.rem(kv, 4)
    c = lax.rem(tp, 2)
    y = lax.div(tp, 2)
    pa = x * (1 - c) + z * c
    pb = z * (1 - c) + x * c

    def kv_of(ia, ib):
        return ia * (1 + 3 * c) + ib * (4 - 3 * c)

    def at_a(g):
        return (kv_of(mod4(pa + g), pb), tp)

    def at_b(g):
        return (kv_of(pa, mod4(pb + g)), tp)

    def kv_peer(i):
        return mod4(z + i // 4) * 4 + mod4(x + i % 4)

    def kv_from(i):
        return mod4(z + 4 - i // 4) * 4 + mod4(x + 4 - i % 4)

    def tp_peer(r):
        return lax.rem(tp + r, 8)

    def tp_from(r):
        return lax.rem(tp + 8 - r, 8)

    def rows48(k):
        return pl.ds(pl.multiple_of(k * 48, 16), 48)

    def rows96(k):
        return pl.ds(pl.multiple_of(k * 96, 32), 96)

    def rows32(k):
        return pl.ds(pl.multiple_of(k * 32, 32), 32)

    sends = []

    def send(*args):
        copy = remote(*args)
        copy.start()
        sends.append(copy)

    loads = [
        pltpu.make_async_copy(tokens, wide_t.at[rows32(tp)], lsem.at[0]),
        pltpu.make_async_copy(w_query, wqkvo.at[:, pl.ds(0, 256)], lsem.at[1]),
        pltpu.make_async_copy(w_key, wqkvo.at[:, pl.ds(256, 256)], lsem.at[2]),
        pltpu.make_async_copy(w_value, wqkvo.at[:, pl.ds(512, 256)], lsem.at[3]),
        pltpu.make_async_copy(w_outgate, wqkvo.at[:, pl.ds(768, 256)], lsem.at[4]),
        pltpu.make_async_copy(w_igate.at[:, pl.ds(pl.multiple_of(kv * 256, 256), 256)], wig_v, lsem.at[5]),
        pltpu.make_async_copy(w_fgate.at[:, pl.ds(pl.multiple_of(kv * 256, 256), 256)], wfg_v, lsem.at[6]),
        pltpu.make_async_copy(state_c, cbuf, lsem.at[7]),
        pltpu.make_async_copy(tail_keys, kbuf, lsem.at[8]),
        pltpu.make_async_copy(tail_values, vbuf, lsem.at[9]),
        pltpu.make_async_copy(w_proj, wproj_v, lsem.at[10]),
        pltpu.make_async_copy(w_gate, wgu.at[pl.ds(0, 256), pl.ds(0, FFD)], lsem.at[11]),
        pltpu.make_async_copy(w_up, wgu.at[pl.ds(0, 256), pl.ds(FFD, FFD)], lsem.at[12]),
        pltpu.make_async_copy(w_down, wdown_v.at[:, pl.ds(0, 256)], lsem.at[13]),
    ]
    for load in loads:
        load.start()

    barrier = pltpu.get_barrier_semaphore()
    for i in range(1, 16):
        pl.semaphore_signal(barrier, inc=1, device_id=(kv_peer(i), tp), device_id_type=MESH)
    for r in range(1, 8):
        pl.semaphore_signal(barrier, inc=1, device_id=(kv, tp_peer(r)), device_id_type=MESH)

    loads[0].wait()
    pl.semaphore_wait(barrier, 22)

    for r in range(1, 8):
        mine = wide_t.at[rows32(tp)]
        send(mine, mine, tok_s.at[r], tok_r.at[r], (kv, tp_peer(r)))

    early, late = (0, 96), (96, 160)

    def weight_rows(slot, part):
        return wgu.at[pl.ds(256 * slot + part[0], part[1])]

    def weight_send(src_slot, dst_slot, part, i, dev):
        send(weight_rows(src_slot, part), weight_rows(dst_slot, part), ws_s.at[i], ws_r.at[i], dev)

    def weight_wait(slot, part, i):
        dst = weight_rows(slot, part)
        remote(dst, dst, ws_s.at[i], ws_r.at[i], (kv, tp)).wait_recv()

    loads[11].wait()
    loads[12].wait()
    weight_send(0, 1, early, 0, at_a(1))
    weight_send(0, 3, early, 1, at_a(3))
    lane = lax.broadcasted_iota(jnp.int32, (128, 128), 1)
    for i in range(5, 7):
        loads[i].wait()
    grow = lax.broadcasted_iota(jnp.int32, (128, 16), 0)
    gcol = lax.broadcasted_iota(jnp.int32, (128, 16), 1)
    pick_i = jnp.where((grow < 2) & (gcol == 2 * tp + grow), 1.0, 0.0).astype(BF)
    pick_f = jnp.where((grow >= 2) & (grow < 4) & (gcol == 2 * tp + grow - 2), 1.0, 0.0).astype(BF)
    gate_w = (
        jnp.dot(pick_i, wig_v[...], preferred_element_type=F32)
        + jnp.dot(pick_f, wfg_v[...], preferred_element_type=F32)
    ).T.astype(BF)
    rows_v[...] = jnp.zeros((8, 128), F32)
    rows_v[0:2, 0:48] = block_forget[...]
    rows_v[2:4, 0:48] = state_m[...]
    rows_v[4:5, 0:48] = lengths[...].astype(F32)
    lane8 = lax.broadcasted_iota(jnp.int32, (8, 128), 1)

    def pair_row(first, second):
        a8 = jnp.broadcast_to(first, (8, 128))
        b8 = jnp.broadcast_to(second, (8, 128))
        return jnp.where(lane8 < 64, a8, pltpu.roll(b8, 64, 1))

    forget_row = pair_row(rows_v[0:1, :], rows_v[1:2, :])
    state_row = pair_row(rows_v[2:3, :], rows_v[3:4, :])
    length_row = pair_row(rows_v[4:5, :], rows_v[4:5, :])[0:1]
    bias_row = jnp.where(lane8 < 64, forget_bias[0], forget_bias[1])
    tg_v[...] = jnp.zeros((128, 128), F32)
    tg_v[0:48, 0:64] = tail_gate[:, 0, :]
    tg_v[64:112, 0:64] = tail_gate[:, 1, :]
    gate_t = tg_v[...].T[:64]
    lane64 = lax.broadcasted_iota(jnp.int32, (64, 128), 1)

    for r in range(1, 8):
        src = wide_t.at[rows32(tp_from(r))]
        remote(src, src, tok_s.at[r], tok_r.at[r], (kv, tp)).wait_recv()
    for b in range(6):
        block = wide_t[:, 128 * b : 128 * b + 128].astype(F32).T
        wide[128 * b : 128 * b + 128, :] = block.astype(BF)
        scaled[128 * b : 128 * b + 128, :] = (block * norm_gain[...]).astype(BF)

    def ring(base, p, own, inn, comb, from_l, from_r, q, qin, qcomb, ql, qr, p_wide, q_wide, ss, rs):
        half = NH // 2
        first, second = pl.ds(0, half), pl.ds(half, half)

        def group(g, *outs):
            ia = mod4(pa + g)
            rows = jnp.concatenate([scaled[rows48(kv_of(ia, ib)), :] for ib in range(4)], axis=0)
            for t, out_ref in enumerate(outs):
                value = jnp.dot(
                    rows, wqkvo[:, base + half * t : base + half * t + half], preferred_element_type=F32
                )
                out_ref[...] = value.astype(out_ref.dtype)

        def waited(dst, i):
            remote(dst, dst, ss.at[i], rs.at[i], (kv, tp)).wait_recv()

        def total(g, put):
            start = mod4(pb + g) * 48
            for i in range(3):
                rows = pl.ds(pl.multiple_of(start + 16 * i, 16), 16)
                put(
                    pl.ds(16 * i, 16),
                    own[rows, :] + from_l[rows, :].astype(F32) + from_r[rows, :].astype(F32),
                )

        def into_q(j, i=None):
            def put(rows, value):
                q[j, rows, :] = value.astype(BF)
                if i is not None:
                    q_wide[i, rows, :] = value[:, half * i : half * i + half]

            return put

        class Stages:
            def opposite(self):
                group(2, p.at[0, :, first], p.at[0, :, second])
                send(p.at[0, :, first], inn.at[0], ss.at[0], rs.at[0], at_a(1))
                send(p.at[0, :, second], inn.at[1], ss.at[1], rs.at[1], at_a(3))

            def plain(self):
                group(1, p_wide.at[0], p.at[1, :, second])
                send(p.at[1, :, second], from_l.at[:, second], ss.at[2], rs.at[2], at_a(1))
                group(3, p.at[2, :, first], p_wide.at[1])
                send(p.at[2, :, first], from_r.at[:, first], ss.at[3], rs.at[3], at_a(3))

            def joined(self):
                waited(inn.at[0], 0)
                comb[0] = (p_wide[0] + inn[0].astype(F32)).astype(BF)
                send(comb.at[0], from_l.at[:, first], ss.at[4], rs.at[4], at_a(1))
                waited(inn.at[1], 1)
                comb[1] = (p_wide[1] + inn[1].astype(F32)).astype(BF)
                send(comb.at[1], from_r.at[:, second], ss.at[5], rs.at[5], at_a(3))

            def mine(self):
                group(0, own.at[:, first], own.at[:, second])

            def across(self):
                waited(from_l.at[:, second], 2)
                waited(from_r.at[:, first], 3)
                waited(from_l.at[:, first], 4)
                waited(from_r.at[:, second], 5)
                total(2, into_q(0))
                send(q.at[0, :, first], qin.at[0], ss.at[6], rs.at[6], at_b(1))
                send(q.at[0, :, second], qin.at[1], ss.at[7], rs.at[7], at_b(3))
                total(1, into_q(1, 0))
                send(q.at[1, :, second], ql.at[:, second], ss.at[8], rs.at[8], at_b(1))
                total(3, into_q(2, 1))
                send(q.at[2, :, first], qr.at[:, first], ss.at[9], rs.at[9], at_b(3))

            def across_joined(self):
                waited(qin.at[0], 6)
                qcomb[0] = (q_wide[0] + qin[0].astype(F32)).astype(BF)
                send(qcomb.at[0], ql.at[:, first], ss.at[10], rs.at[10], at_b(1))
                waited(qin.at[1], 7)
                qcomb[1] = (q_wide[1] + qin[1].astype(F32)).astype(BF)
                send(qcomb.at[1], qr.at[:, second], ss.at[11], rs.at[11], at_b(3))

            def result(self):
                here = pl.ds(pl.multiple_of(pb * 48, 16), 48)
                waited(ql.at[:, second], 8)
                waited(qr.at[:, first], 9)
                waited(ql.at[:, first], 10)
                waited(qr.at[:, second], 11)
                return (
                    own[here, :]
                    + from_l[here, :].astype(F32)
                    + from_r[here, :].astype(F32)
                    + ql[...].astype(F32)
                    + qr[...].astype(F32)
                )

        return Stages()

    def small_sum(recv_ref, own_tile, ss, rs):
        acc = own_tile
        for i in range(1, 16):
            remote(recv_ref.at[i], recv_ref.at[i], ss.at[i], rs.at[i], (kv, tp)).wait_recv()
            acc = acc + recv_ref[i]
        return acc

    lane48 = lax.broadcasted_iota(jnp.int32, (48, 128), 1)

    def gate_tiles():
        def step(k, _):
            rows = rows48(k)
            part = jnp.dot(scaled[rows, :], gate_w, preferred_element_type=F32)
            wf = wide[rows, :].astype(F32)
            sq = jnp.sum(wf * wf, axis=1, keepdims=True)
            gsend[k] = transpose_padded(jnp.where(lane48 == 4, sq, part))[:8]
            return 0

        lax.fori_loop(0, 16, step, 0, unroll=4)
        for i in range(1, 16):
            k = kv_peer(i)
            send(gsend.at[k], grecv.at[i], g_s.at[i], g_r.at[i], (k, tp))

    for i in range(1, 5):
        loads[i].wait()
    qk = ring(0, *qk_bufs, qk_s, qk_r)
    vo = ring(NH, *vo_bufs, vo_s, vo_r)
    qk.opposite()
    qk.plain()
    vo.opposite()
    gate_tiles()
    qk.joined()
    vo.plain()
    vo.joined()
    weight_send(0, 1, late, 2, at_a(1))
    weight_send(0, 3, late, 3, at_a(3))
    qk.mine()
    vo.mine()
    qk.across()
    qk.across_joined()
    vo.across()
    gsum = small_sum(grecv, gsend[kv], g_s, g_r)
    inv_row = lax.rsqrt(gsum[4:5, :] / D + EPS)
    inv_col = column_of(inv_row)[:48]
    igate = pair_row(gsum[0:1, :] * inv_row, gsum[1:2, :] * inv_row)
    fpre = pair_row(gsum[2:3, :] * inv_row, gsum[3:4, :] * inv_row) + bias_row
    log_sig = -(jnp.maximum(-fpre, 0.0) + jnp.log1p(jnp.exp(-jnp.abs(fpre))))
    running = forget_row + log_sig
    inter = running + state_row
    pos = lax.broadcasted_iota(jnp.int32, (64, 128), 0).astype(F32)
    tail_log = jnp.where(pos < length_row, running[0:1] + gate_t, -jnp.inf)
    top = jnp.maximum(jnp.maximum(inter[0:1], jnp.max(tail_log, axis=0, keepdims=True)), igate[0:1])
    w_inter = jnp.exp(inter[0:1] - top)
    w_own = column_of(jnp.exp(igate[0:1] - top))
    w_tail = jnp.exp(tail_log - top)

    qk_sum = qk.result()
    for h in range(2):
        qs[h] = qk_sum[:, 128 * h : 128 * h + 128] * inv_col
    for i in range(7, 10):
        loads[i].wait()

    for h in range(2):
        q_hi = qs[h].astype(BF).astype(F32)
        q_lo = (qs[h] - q_hi).astype(BF).astype(F32)
        q_rows[:, 2 * h, :] = jnp.concatenate([q_hi, q_hi], axis=1)
        q_rows[:, 2 * h + 1, :] = jnp.concatenate([q_lo, jnp.zeros((48, 128), F32)], axis=1)
    for i in range(4, 8):
        q_rows[:, i, :] = jnp.zeros((48, 256), F32)
    contract_last = (((1,), (1,)), ((), ()))
    lane1 = lax.broadcasted_iota(jnp.int32, (1, 128), 1)

    def recall_step(s, _):
        lhs = q_rows[s].astype(BF)
        state = cbuf[s].reshape(256, 128)
        s_hi = state.astype(BF)
        s_lo = (state - s_hi.astype(F32)).astype(BF)
        m = lax.dot_general(
            lhs, jnp.concatenate([s_hi, s_lo], axis=1), contract_last, preferred_element_type=F32
        )
        mem_n[0, pl.ds(s, 1), :] = m[0:1, :128] + m[1:2, :128]
        mem_n[1, pl.ds(s, 1), :] = m[2:3, 128:] + m[3:4, 128:]
        sc = lax.dot_general(
            lhs[:, :128], kbuf[s].reshape(128, 128), contract_last, preferred_element_type=F32
        )
        sc_n[pl.ds(s, 1), :] = jnp.where(lane1 < 64, sc[0:1] + sc[1:2], sc[2:3] + sc[3:4])
        return 0

    lax.fori_loop(0, 24, recall_step, 0, unroll=4)
    vo.across_joined()
    lax.fori_loop(24, 48, recall_step, 0, unroll=4)
    sc_r = transpose_padded(sc_n[...])
    sc_t = jnp.where(lane64 < 64, sc_r[:64], pltpu.roll(sc_r[64:], 64, 1))
    weighted = w_tail * (sc_t * 128 ** (-0.5))
    rows_w = jnp.concatenate([weighted, weighted], axis=0).T
    prow = lax.broadcasted_iota(jnp.int32, (128, 256), 0)
    plane = lax.broadcasted_iota(jnp.int32, (128, 256), 1)
    slot = 2 * lax.rem(prow, 2) + lax.div(prow, 64)
    rows_w = jnp.where(lax.div(plane, 64) == slot, jnp.concatenate([rows_w, rows_w], axis=1), 0.0)
    w_hi = rows_w.astype(BF)
    w_lo = (rows_w - w_hi.astype(F32)).astype(BF)
    step_of = lax.div(lax.rem(prow, 64), 2)

    def tail_step(g, acc):
        here = jnp.where(step_of == g, 1.0, 0.0).astype(BF)
        vals = vbuf[pl.ds(2 * g, 2)].reshape(256, 128)
        return (
            acc
            + jnp.dot(w_hi * here, vals, preferred_element_type=F32)
            + jnp.dot(w_lo * here, vals, preferred_element_type=F32)
        )

    tail_part = lax.fori_loop(0, 24, tail_step, jnp.zeros((128, 128), F32), unroll=4)
    w_state = column_of(w_inter)
    vo_sum = vo.result()
    mixed = []
    for h in range(2):
        q = qs[h]
        k = qk_sum[:, 256 + 128 * h : 384 + 128 * h] * inv_col * 128 ** (-0.5)
        v = vo_sum[:, 128 * h : 128 * h + 128] * inv_col
        og = vo_sum[:, 256 + 128 * h : 384 + 128 * h] * inv_col
        own = jnp.sum(q * k, axis=1, keepdims=True)
        rows = slice(64 * h, 64 * h + 48)
        recalled = mem_n[h] * w_state[rows] + tail_part[rows] + w_own[rows] * own * v
        ms = jnp.mean(recalled * recalled, axis=1, keepdims=True)
        normed = recalled * lax.rsqrt(ms + EPS)
        hg = head_gain[:, 128 * h : 128 * h + 128]
        mixed.append((normed * hg * (1.0 / (1.0 + jnp.exp(-og)))).astype(BF))
    mix_all[rows48(kv), :] = jnp.concatenate(mixed, axis=1)
    for i in range(1, 16):
        mine = mix_all.at[rows48(kv)]
        send(mine, mine, mix_s.at[i], mix_r.at[i], (kv_peer(i), tp))
    loads[10].wait()
    for i in range(1, 16):
        src = mix_all.at[rows48(kv_from(i))]
        remote(src, src, mix_s.at[i], mix_r.at[i], (kv, tp)).wait_recv()

    weight_wait(1, early, 0)
    weight_wait(1, late, 2)
    weight_send(1, 2, (0, 128), 4, at_a(1))
    weight_wait(3, early, 1)
    weight_wait(3, late, 3)
    weight_send(3, 2, (128, 128), 5, at_a(3))
    for r in [4, 3, 5, 2, 6, 1, 7, 0]:
        part = jnp.dot(mix_all[rows96(tp_peer(r)), :], wproj_v[...], preferred_element_type=F32)
        att_send[r] = part.astype(BF)
        if r:
            send(att_send.at[r], att_recv.at[r], att_s.at[r], att_r.at[r], (kv, tp_peer(r)))
    attended = att_send[0].astype(F32)
    for r in range(1, 8):
        remote(att_recv.at[r], att_recv.at[r], att_s.at[r], att_r.at[r], (kv, tp)).wait_recv()
        attended = attended + att_recv[r].astype(F32)
    middle = (wide[rows96(tp), :].astype(F32) + attended).astype(BF)
    mid_all[rows96(tp), :] = middle
    middle_f = middle.astype(F32)
    sm_block = (middle_f * mixer_gain[...]).astype(BF)
    later = []

    def send_unless(here, *args):
        copy = remote(*args)

        @pl.when(jnp.logical_not(here))
        def _():
            copy.start()

        later.append((here, copy))

    for i in range(2):
        sm_own[i] = sm_block[48 * i : 48 * i + 48]
    for n, (dy, dc, i) in enumerate((dy, dc, i) for dy in (2, 1, 3, 0) for dc in range(2) for i in range(2)):
        k = 2 * tp + i
        kz, kx = lax.div(k, 4), lax.rem(k, 4)
        cd = lax.rem(c + dc, 2)
        dev_kv = (1 - cd) * (4 * z + kx) + cd * (4 * kz + x)
        ra = mod4((1 - cd) * (kx + 4 - x) + cd * (kz + 4 - z))
        ib = (1 - cd) * kz + cd * kx
        args = (
            sm_own.at[i], lhs4.at[ra, rows48(ib)], sm_s.at[n], sm_r.at[ra * 4 + ib],
            (dev_kv, 2 * mod4(y + dy) + cd),
        )
        if dy == 0 and dc == 0:
            send_unless(dev_kv == kv, *args)
        else:
            send(*args)
    for i in range(2):
        sq = middle_f[48 * i : 48 * i + 48]
        sq = sq * sq
        row = jnp.sum(transpose_padded(sq[:, :128] + sq[:, 128:]), axis=0, keepdims=True)
        ssend[i] = jnp.broadcast_to(row, (8, 128))
        k = 2 * tp + i
        slot = 4 * mod4(lax.div(k, 4) + 4 - z) + mod4(lax.rem(k, 4) + 4 - x)
        for r in range(8):
            args = (ssend.at[i], srecv.at[slot], sq_s.at[8 * i + r], sq_r.at[slot], (k, tp_peer(r)))
            if r == 0:
                send_unless(k == kv, *args)
            else:
                send(*args)
    def down_weights(slot, part=(0, FFD)):
        return wdown_v.at[pl.ds(part[0], part[1]), pl.ds(256 * slot, 256)]

    def down_send(src_slot, dst_slot, part, i, dev):
        send(down_weights(src_slot, part), down_weights(dst_slot, part), wd_s.at[i], wd_r.at[i], dev)

    def down_got(slot, part, i):
        dst = down_weights(slot, part)
        remote(dst, dst, wd_s.at[i], wd_r.at[i], (kv, tp)).wait_recv()

    whole, upper, lower = (0, FFD), (0, FFD // 2), (FFD // 2, FFD // 2)
    loads[13].wait()
    down_send(0, 1, whole, 0, at_a(1))
    down_send(0, 3, whole, 1, at_a(3))
    for r in [4, 3, 5, 2, 6, 1, 7]:
        mine = mid_all.at[rows96(tp)]
        send(mine, mine, mid_s.at[r], mid_r.at[r], (kv, tp_peer(r)))

    for n in (4, 5):
        weight_wait(2, (128 * (n - 4), 128), n)
    for ra in range(4):
        for ib in range(4):
            dst = lhs4.at[ra, pl.ds(48 * ib, 48)]
            got = remote(dst, dst, sm_s.at[0], sm_r.at[ra * 4 + ib], (kv, tp))
            if ra:
                got.wait_recv()
            else:
                k = kv_of(pa, ib)
                here = lax.div(k, 2) == tp

                @pl.when(jnp.logical_not(here))
                def _():
                    got.wait_recv()

                @pl.when(here)
                def _():
                    lhs4[0, 48 * ib : 48 * ib + 48, :] = sm_own[lax.rem(k, 2)]
    rows_all = jnp.concatenate([lhs4[ra] for ra in range(4)], axis=1)
    first, second = pl.ds(0, FFD), pl.ds(FFD, FFD)

    def half_product(base):
        def step(t, _):
            cols = pl.ds(pl.multiple_of(base + t * 256, 128), 256)
            b_own[:, cols] = jnp.dot(rows_all, wgu[:, cols], preferred_element_type=F32)
            return 0

        lax.fori_loop(0, 5, step, 0, unroll=True)
        cols = pl.ds(base + 1280, 128)
        b_own[:, cols] = jnp.dot(rows_all, wgu[:, cols], preferred_element_type=F32)

    def b_rows(g):
        return pl.ds(pl.multiple_of(mod4(pb + g) * 48, 16), 48)

    def b_put(j, g, cols):
        b_q[j, :, cols] = b_own[b_rows(g), cols].astype(BF)

    def b_wait(dst, i):
        remote(dst, dst, rb_s.at[i], rb_r.at[i], (kv, tp)).wait_recv()

    right, left = at_b(1), at_b(3)
    half_product(0)
    b_put(0, 2, first)
    send(b_q.at[0, :, first], b_qin.at[0], rb_s.at[6], rb_r.at[6], right)
    b_put(2, 3, first)
    send(b_q.at[2, :, first], b_qr.at[:, first], rb_s.at[9], rb_r.at[9], left)
    half_product(FFD)
    b_put(0, 2, second)
    send(b_q.at[0, :, second], b_qin.at[1], rb_s.at[7], rb_r.at[7], left)
    b_put(1, 1, second)
    send(b_q.at[1, :, second], b_ql.at[:, second], rb_s.at[8], rb_r.at[8], right)
    b_wait(b_qin.at[0], 6)
    b_qcomb[0] = (b_own[b_rows(1), first] + b_qin[0].astype(F32)).astype(BF)
    send(b_qcomb.at[0], b_ql.at[:, first], rb_s.at[10], rb_r.at[10], right)
    b_wait(b_qin.at[1], 7)
    b_qcomb[1] = (b_own[b_rows(3), second] + b_qin[1].astype(F32)).astype(BF)
    send(b_qcomb.at[1], b_qr.at[:, second], rb_s.at[11], rb_r.at[11], left)
    for r in range(1, 8):
        src = mid_all.at[rows96(tp_from(r))]
        remote(src, src, mid_s.at[r], mid_r.at[r], (kv, tp)).wait_recv()
    srow = lax.broadcasted_iota(jnp.int32, (32, 256), 0)
    scol = lax.broadcasted_iota(jnp.int32, (32, 256), 1)
    pick = jnp.where(scol == 32 * tp + srow, 1.0, 0.0).astype(BF)
    mid_sel[...] = lax.dot_general(
        pick, mid_all[...], (((1,), (1,)), ((), ())), preferred_element_type=F32
    )
    sq_here = lax.div(kv, 2) == tp
    sq0 = remote(srecv.at[0], srecv.at[0], sq_s.at[0], sq_r.at[0], (kv, tp))

    @pl.when(jnp.logical_not(sq_here))
    def _():
        sq0.wait_recv()

    @pl.when(sq_here)
    def _():
        srecv[0] = ssend[lax.rem(kv, 2)]

    ssum = small_sum(srecv, srecv[0], sq_s, sq_r)
    inv_mid = column_of(lax.rsqrt(ssum[0:1] / D + EPS))[:48]
    b_wait(b_ql.at[:, second], 8)
    b_wait(b_qr.at[:, first], 9)
    b_wait(b_ql.at[:, first], 10)
    b_wait(b_qr.at[:, second], 11)

    def both(cols):
        return b_own[b_rows(0), cols] + b_ql[:, cols].astype(F32) + b_qr[:, cols].astype(F32)

    def hidden_step(t, _):
        cols = pl.ds(pl.multiple_of(t * 128, 128), 128)
        gate = both(cols) * inv_mid
        up = both(pl.ds(pl.multiple_of(t * 128 + FFD, 128), 128)) * inv_mid
        hid[rows48(pb), cols] = (gate * (1.0 / (1.0 + jnp.exp(-gate))) * up).astype(BF)
        return 0

    lax.fori_loop(0, FFD // 128, hidden_step, 0)

    def chunk(rb, part=(0, 48)):
        return hid.at[pl.ds(pl.multiple_of(mod4(pb + 4 - rb) * 48 + part[0], 16), part[1])]

    def hop(ref, i, dev):
        send(ref, ref, h_s.at[i], h_r.at[i], dev)

    def arrived(ref, i):
        remote(ref, ref, h_s.at[i], h_r.at[i], (kv, tp)).wait_recv()

    hop(chunk(0), 0, at_b(1))
    hop(chunk(0), 1, at_b(3))
    down_got(1, whole, 0)
    down_send(1, 2, upper, 2, at_a(1))
    down_got(3, whole, 1)
    down_send(3, 2, lower, 3, at_a(3))
    arrived(chunk(1), 0)
    hop(chunk(1, (0, 32)), 2, at_b(1))
    arrived(chunk(3), 1)
    hop(chunk(3, (32, 16)), 3, at_b(3))
    down_got(2, upper, 2)
    down_got(2, lower, 3)
    arrived(chunk(2, (0, 32)), 2)
    arrived(chunk(2, (32, 16)), 3)

    lane16 = lax.broadcasted_iota(jnp.int32, (8, 16, 128), 2)
    for ra in (2, 1, 3, 0):
        part = jnp.dot(hid[...], wdown_v[:, 256 * ra : 256 * ra + 256], preferred_element_type=F32)
        part = jnp.concatenate([part, jnp.zeros((64, 256), F32)], axis=0).T
        tail = part[:, 128:].reshape(8, 2, 16, 128)
        tail = jnp.where(lane16 < 64, tail[:, 0], pltpu.roll(tail[:, 1], 64, 2))
        fsend[ra, :, 0:32, :] = part[:, :128].reshape(8, 32, 128).astype(BF)
        fsend[ra, :, 32:48, :] = tail.astype(BF)
        for dy in (2, 1, 3, 0):
            for dc in range(2):
                t = 2 * mod4(y + dy) + lax.rem(c + dc, 2)
                if ra or dy or dc:
                    send(
                        fsend.at[ra, t], frecv.at[c, ra, dy], f_s.at[8 * ra + 2 * dy + dc],
                        f_r.at[16 * c + 4 * ra + dy], (kv_of(mod4(pa + 4 - ra), pb), t),
                    )
    frecv[c, 0, 0] = fsend[0, tp]
    other = frecv.at[1 - c, 0, 0]
    remote(other, other, f_s.at[0], f_r.at[16 * (1 - c)], (kv, tp)).wait_recv()
    for cs in range(2):
        mains, tails = [], []
        for ra in range(4):
            piece = 0.0
            for dy in range(4):
                dst = frecv.at[cs, ra, dy]
                if ra or dy:
                    remote(dst, dst, f_s.at[0], f_r.at[16 * cs + 4 * ra + dy], (kv, tp)).wait_recv()
                piece = piece + frecv[cs, ra, dy].astype(F32)
            mains.append(piece[:32])
            tails += [piece[32:], pltpu.roll(piece[32:], 64, 1)]
        by_seq = jnp.concatenate(
            [jnp.concatenate(mains, axis=0).T, jnp.concatenate(tails, axis=0).T[:64]], axis=0
        )
        for ra in range(4):
            block = pltpu.roll(by_seq, (128 - 32 * ra) % 128, 1) if ra else by_seq
            for ib in range(4):
                k = 4 * ib + mod4(x + ra) if cs == 0 else 4 * mod4(z + ra) + ib
                mine = block[48 * ib : 48 * ib + 48]
                if cs == 0:
                    down_rows[rows48(k), :] = mine
                else:
                    down_rows[rows48(k), :] += mine
    for b in range(6):
        cols = slice(128 * b, 128 * b + 128)
        out[:, cols] = (mid_sel[:, cols] + down_rows[cols, :].T[:32]).astype(BF)
    for copy in sends:
        copy.wait_send()
    for here, copy in later:
        @pl.when(jnp.logical_not(here))
        def _():
            copy.wait_send()


def per_device(
    tokens, norm_gain, w_query, w_key, w_value, w_outgate, w_igate, w_fgate, forget_bias, head_gain,
    w_proj, mixer_gain, w_gate, w_up, w_down, state_c, state_m, tail_keys, tail_values, tail_gate,
    block_forget, lengths,
):
    any_spec = pl.BlockSpec(memory_space=pl.ANY)
    vm_spec = pl.BlockSpec(memory_space=pltpu.VMEM)
    dma = pltpu.SemaphoreType.DMA

    def ring_bufs(n):
        return [
            pltpu.VMEM((3, 192, n), BF),
            pltpu.VMEM((192, n), F32),
            pltpu.VMEM((2, 192, n // 2), BF),
            pltpu.VMEM((2, 192, n // 2), BF),
            pltpu.VMEM((192, n), BF),
            pltpu.VMEM((192, n), BF),
            pltpu.VMEM((3, 48, n), BF),
            pltpu.VMEM((2, 48, n // 2), BF),
            pltpu.VMEM((2, 48, n // 2), BF),
            pltpu.VMEM((48, n), BF),
            pltpu.VMEM((48, n), BF),
            pltpu.VMEM((2, 192, n // 2), F32),
            pltpu.VMEM((2, 48, n // 2), F32),
        ]

    scratch = [
        pltpu.VMEM((256, 768), BF),
        pltpu.VMEM((768, 256), BF),
        pltpu.VMEM((768, 256), BF),
        pltpu.VMEM((256, N1), BF),
        pltpu.VMEM((16, 256), BF),
        pltpu.VMEM((16, 256), BF),
        pltpu.VMEM((256, 256), BF),
        pltpu.VMEM((1024, N2), BF),
        pltpu.VMEM((FFD, 1024), BF),
        pltpu.VMEM((48, 2, 128, 128), F32),
        pltpu.VMEM((48, 2, 64, 128), BF),
        pltpu.VMEM((48, 2, 64, 128), BF),
        pltpu.VMEM((16, 8, 128), F32),
        pltpu.VMEM((16, 8, 128), F32),
        pltpu.VMEM((8, 128), F32),
        pltpu.VMEM((128, 128), F32),
        *ring_bufs(NH),
        *ring_bufs(NH),
        pltpu.VMEM((2, 48, 128), F32),
        pltpu.VMEM((48, 8, 256), F32),
        pltpu.VMEM((2, 48, 128), F32),
        pltpu.VMEM((48, 128), F32),
        pltpu.VMEM((768, 256), BF),
        pltpu.VMEM((8, 96, 256), BF),
        pltpu.VMEM((8, 96, 256), BF),
        pltpu.VMEM((768, 256), BF),
        pltpu.VMEM((2, 8, 128), F32),
        pltpu.VMEM((16, 8, 128), F32),
        pltpu.VMEM((32, 768), F32),
        pltpu.VMEM((4, 192, 256), BF),
        pltpu.VMEM((2, 48, 256), BF),
        pltpu.VMEM((192, N2), F32),
        *ring_bufs(N2)[6:11],
        pltpu.VMEM((192, FFD), BF),
        pltpu.VMEM((4, 8, 48, 128), BF),
        pltpu.VMEM((2, 4, 4, 48, 128), BF),
        pltpu.VMEM((768, 128), F32),
        dma((14,)),
        dma((8,)), dma((8,)),
        dma((16,)), dma((16,)),
        dma((16,)), dma((16,)),
        dma((8,)), dma((8,)),
        dma((8,)), dma((8,)),
        dma((16,)), dma((16,)),
        dma((12,)), dma((12,)),
        dma((12,)), dma((12,)),
        dma((12,)), dma((12,)),
        dma((6,)), dma((6,)),
        dma((16,)), dma((16,)),
        dma((4,)), dma((4,)),
        dma((4,)), dma((4,)),
        dma((32,)), dma((32,)),
    ]
    specs = [any_spec] * 21
    for i in (1, 8, 10, 17, 18, 19, 20):
        specs[i] = vm_spec
    specs.append(pl.BlockSpec(memory_space=pltpu.SMEM))
    result_t = pl.pallas_call(
        layer,
        out_shape=jax.ShapeDtypeStruct((32, 768), BF),
        in_specs=specs,
        out_specs=vm_spec,
        scratch_shapes=scratch,
        compiler_params=pltpu.CompilerParams(
            collective_id=0, has_side_effects=True, vmem_limit_bytes=60 * 1024 * 1024
        ),
    )(
        tokens.T, norm_gain.reshape(1, 256), w_query, w_key, w_value, w_outgate, w_igate.T, w_fgate.T,
        head_gain.reshape(1, 256), w_proj, mixer_gain.reshape(1, 256), w_gate, w_up, w_down,
        state_c, tail_keys, tail_values, tail_gate, state_m.T, block_forget.T, lengths.reshape(1, 48), forget_bias,
    )
    return result_t.T


def solution(mesh):
    kvtp = P("kv", "tp")
    return jax.shard_map(
        per_device,
        mesh=mesh,
        in_specs=(
            P(None, ("kv", "tp")), P("kv"), kvtp, kvtp, kvtp, kvtp, P(), P(), P("tp"), P("tp"),
            P("tp", "kv"), P("kv"), kvtp, kvtp, P("tp", "kv"), P("kv", "tp", None, None), kvtp,
            P("kv", "tp", None, None), P("kv", "tp", None, None), P("kv", "tp", None), kvtp, P("kv"),
        ),
        out_specs=P(None, ("kv", "tp")),
        check_vma=False,
    )
```

```python
import jax
import jax.numpy as jnp
from jax import lax
from jax.experimental import pallas as pl
from jax.experimental.pallas import tpu as pltpu
from jax.sharding import PartitionSpec as P

D = 4096
EPS = 1e-06
F32 = jnp.float32
BF = jnp.bfloat16
MESH = pl.DeviceIdType.MESH
N1 = 1024
NH = 512
N2 = 2816
FFD = 1408


def remote(src, dst, ss, rs, dev):
    return pltpu.make_async_remote_copy(
        src_ref=src, dst_ref=dst, send_sem=ss, recv_sem=rs, device_id=dev, device_id_type=MESH
    )


def mod4(v):
    return lax.rem(v, 4)


def transpose_padded(rows):
    missing = 128 - rows.shape[0]
    if missing:
        rows = jnp.concatenate([rows, jnp.zeros((missing, rows.shape[1]), F32)], axis=0)
    return rows.T


def column_of(row):
    return jnp.broadcast_to(row, (128, 128)).T


def layer(
    tokens, norm_gain, w_query, w_key, w_value, w_outgate, w_igate, w_fgate, head_gain, w_proj,
    mixer_gain, w_gate, w_up, w_down, state_c, tail_keys, tail_values, tail_gate, state_m, block_forget,
    lengths, forget_bias,
    out,
    wide_t, wide, scaled, wqkvo, wig_v, wfg_v, wproj_v, wgu, wdown_v, cbuf, kbuf, vbuf,
    gsend, grecv, rows_v, tg_v,
    *rest,
):
    qk_bufs, vo_bufs, rest = rest[:13], rest[13:26], rest[26:]
    (
        qs, q_rows, mem_n, sc_n, mix_all, att_send, att_recv, mid_all, ssend, srecv, mid_sel,
        lhs4, sm_own, b_own, b_q, b_qin, b_qcomb, b_ql, b_qr,
        hid, fsend, frecv, down_rows,
        lsem, tok_s, tok_r, g_s, g_r, mix_s, mix_r, att_s, att_r, mid_s, mid_r, sq_s, sq_r,
        qk_s, qk_r, vo_s, vo_r, rb_s, rb_r, ws_s, ws_r, sm_s, sm_r, wd_s, wd_r, h_s, h_r, f_s, f_r,
    ) = rest
    kv = lax.axis_index("kv")
    tp = lax.axis_index("tp")
    z = lax.div(kv, 4)
    x = lax.rem(kv, 4)
    c = lax.rem(tp, 2)
    y = lax.div(tp, 2)
    pa = x * (1 - c) + z * c
    pb = z * (1 - c) + x * c

    def kv_of(ia, ib):
        return ia * (1 + 3 * c) + ib * (4 - 3 * c)

    def at_a(g):
        return (kv_of(mod4(pa + g), pb), tp)

    def at_b(g):
        return (kv_of(pa, mod4(pb + g)), tp)

    def kv_peer(i):
        return mod4(z + i // 4) * 4 + mod4(x + i % 4)

    def kv_from(i):
        return mod4(z + 4 - i // 4) * 4 + mod4(x + 4 - i % 4)

    def tp_peer(r):
        return lax.rem(tp + r, 8)

    def tp_from(r):
        return lax.rem(tp + 8 - r, 8)

    def rows48(k):
        return pl.ds(pl.multiple_of(k * 48, 16), 48)

    def rows96(k):
        return pl.ds(pl.multiple_of(k * 96, 32), 96)

    def rows32(k):
        return pl.ds(pl.multiple_of(k * 32, 32), 32)

    sends = []

    def send(*args):
        copy = remote(*args)
        copy.start()
        sends.append(copy)

    loads = [
        pltpu.make_async_copy(tokens, wide_t.at[rows32(tp)], lsem.at[0]),
        pltpu.make_async_copy(w_query, wqkvo.at[:, pl.ds(0, 256)], lsem.at[1]),
        pltpu.make_async_copy(w_key, wqkvo.at[:, pl.ds(256, 256)], lsem.at[2]),
        pltpu.make_async_copy(w_value, wqkvo.at[:, pl.ds(512, 256)], lsem.at[3]),
        pltpu.make_async_copy(w_outgate, wqkvo.at[:, pl.ds(768, 256)], lsem.at[4]),
        pltpu.make_async_copy(w_igate.at[:, pl.ds(pl.multiple_of(kv * 256, 256), 256)], wig_v, lsem.at[5]),
        pltpu.make_async_copy(w_fgate.at[:, pl.ds(pl.multiple_of(kv * 256, 256), 256)], wfg_v, lsem.at[6]),
        pltpu.make_async_copy(state_c, cbuf, lsem.at[7]),
        pltpu.make_async_copy(tail_keys, kbuf, lsem.at[8]),
        pltpu.make_async_copy(tail_values, vbuf, lsem.at[9]),
        pltpu.make_async_copy(w_proj, wproj_v, lsem.at[10]),
        pltpu.make_async_copy(w_gate, wgu.at[pl.ds(0, 256), pl.ds(0, FFD)], lsem.at[11]),
        pltpu.make_async_copy(w_up, wgu.at[pl.ds(0, 256), pl.ds(FFD, FFD)], lsem.at[12]),
        pltpu.make_async_copy(w_down, wdown_v.at[:, pl.ds(0, 256)], lsem.at[13]),
    ]
    for load in loads:
        load.start()

    barrier = pltpu.get_barrier_semaphore()
    for i in range(1, 16):
        pl.semaphore_signal(barrier, inc=1, device_id=(kv_peer(i), tp), device_id_type=MESH)
    for r in range(1, 8):
        pl.semaphore_signal(barrier, inc=1, device_id=(kv, tp_peer(r)), device_id_type=MESH)

    loads[0].wait()
    pl.semaphore_wait(barrier, 22)

    for r in range(1, 8):
        mine = wide_t.at[rows32(tp)]
        send(mine, mine, tok_s.at[r], tok_r.at[r], (kv, tp_peer(r)))

    early, late = (0, 96), (96, 160)

    def weight_rows(slot, part):
        return wgu.at[pl.ds(256 * slot + part[0], part[1])]

    def weight_send(src_slot, dst_slot, part, i, dev):
        send(weight_rows(src_slot, part), weight_rows(dst_slot, part), ws_s.at[i], ws_r.at[i], dev)

    def weight_wait(slot, part, i):
        dst = weight_rows(slot, part)
        remote(dst, dst, ws_s.at[i], ws_r.at[i], (kv, tp)).wait_recv()

    loads[11].wait()
    loads[12].wait()
    weight_send(0, 1, early, 0, at_a(1))
    weight_send(0, 3, early, 1, at_a(3))
    lane = lax.broadcasted_iota(jnp.int32, (128, 128), 1)
    for i in range(5, 7):
        loads[i].wait()
    grow = lax.broadcasted_iota(jnp.int32, (128, 16), 0)
    gcol = lax.broadcasted_iota(jnp.int32, (128, 16), 1)
    pick_i = jnp.where((grow < 2) & (gcol == 2 * tp + grow), 1.0, 0.0).astype(BF)
    pick_f = jnp.where((grow >= 2) & (grow < 4) & (gcol == 2 * tp + grow - 2), 1.0, 0.0).astype(BF)
    gate_w = (
        jnp.dot(pick_i, wig_v[...], preferred_element_type=F32)
        + jnp.dot(pick_f, wfg_v[...], preferred_element_type=F32)
    ).T.astype(BF)
    rows_v[...] = jnp.zeros((8, 128), F32)
    rows_v[0:2, 0:48] = block_forget[...]
    rows_v[2:4, 0:48] = state_m[...]
    rows_v[4:5, 0:48] = lengths[...].astype(F32)
    lane8 = lax.broadcasted_iota(jnp.int32, (8, 128), 1)

    def pair_row(first, second):
        a8 = jnp.broadcast_to(first, (8, 128))
        b8 = jnp.broadcast_to(second, (8, 128))
        return jnp.where(lane8 < 64, a8, pltpu.roll(b8, 64, 1))

    forget_row = pair_row(rows_v[0:1, :], rows_v[1:2, :])
    state_row = pair_row(rows_v[2:3, :], rows_v[3:4, :])
    length_row = pair_row(rows_v[4:5, :], rows_v[4:5, :])[0:1]
    bias_row = jnp.where(lane8 < 64, forget_bias[0], forget_bias[1])
    tg_v[...] = jnp.zeros((128, 128), F32)
    tg_v[0:48, 0:64] = tail_gate[:, 0, :]
    tg_v[64:112, 0:64] = tail_gate[:, 1, :]
    gate_t = tg_v[...].T[:64]
    lane64 = lax.broadcasted_iota(jnp.int32, (64, 128), 1)

    for r in range(1, 8):
        src = wide_t.at[rows32(tp_from(r))]
        remote(src, src, tok_s.at[r], tok_r.at[r], (kv, tp)).wait_recv()
    for b in range(6):
        block = wide_t[:, 128 * b : 128 * b + 128].astype(F32).T
        wide[128 * b : 128 * b + 128, :] = block.astype(BF)
        scaled[128 * b : 128 * b + 128, :] = (block * norm_gain[...]).astype(BF)

    def ring(base, p, own, inn, comb, from_l, from_r, q, qin, qcomb, ql, qr, p_wide, q_wide, ss, rs):
        half = NH // 2
        first, second = pl.ds(0, half), pl.ds(half, half)

        def group(g, *outs):
            ia = mod4(pa + g)
            rows = jnp.concatenate([scaled[rows48(kv_of(ia, ib)), :] for ib in range(4)], axis=0)
            for t, out_ref in enumerate(outs):
                value = jnp.dot(
                    rows, wqkvo[:, base + half * t : base + half * t + half], preferred_element_type=F32
                )
                out_ref[...] = value.astype(out_ref.dtype)

        def waited(dst, i):
            remote(dst, dst, ss.at[i], rs.at[i], (kv, tp)).wait_recv()

        def total(g, put):
            start = mod4(pb + g) * 48
            for i in range(3):
                rows = pl.ds(pl.multiple_of(start + 16 * i, 16), 16)
                put(
                    pl.ds(16 * i, 16),
                    own[rows, :] + from_l[rows, :].astype(F32) + from_r[rows, :].astype(F32),
                )

        def into_q(j, i=None):
            def put(rows, value):
                q[j, rows, :] = value.astype(BF)
                if i is not None:
                    q_wide[i, rows, :] = value[:, half * i : half * i + half]

            return put

        class Stages:
            def opposite(self):
                group(2, p.at[0, :, first], p.at[0, :, second])
                send(p.at[0, :, first], inn.at[0], ss.at[0], rs.at[0], at_a(1))
                send(p.at[0, :, second], inn.at[1], ss.at[1], rs.at[1], at_a(3))

            def plain(self):
                group(1, p_wide.at[0], p.at[1, :, second])
                send(p.at[1, :, second], from_l.at[:, second], ss.at[2], rs.at[2], at_a(1))
                group(3, p.at[2, :, first], p_wide.at[1])
                send(p.at[2, :, first], from_r.at[:, first], ss.at[3], rs.at[3], at_a(3))

            def joined(self):
                waited(inn.at[0], 0)
                comb[0] = (p_wide[0] + inn[0].astype(F32)).astype(BF)
                send(comb.at[0], from_l.at[:, first], ss.at[4], rs.at[4], at_a(1))
                waited(inn.at[1], 1)
                comb[1] = (p_wide[1] + inn[1].astype(F32)).astype(BF)
                send(comb.at[1], from_r.at[:, second], ss.at[5], rs.at[5], at_a(3))

            def mine(self):
                group(0, own.at[:, first], own.at[:, second])

            def across(self):
                waited(from_l.at[:, second], 2)
                waited(from_r.at[:, first], 3)
                waited(from_l.at[:, first], 4)
                waited(from_r.at[:, second], 5)
                total(2, into_q(0))
                send(q.at[0, :, first], qin.at[0], ss.at[6], rs.at[6], at_b(1))
                send(q.at[0, :, second], qin.at[1], ss.at[7], rs.at[7], at_b(3))
                total(1, into_q(1, 0))
                send(q.at[1, :, second], ql.at[:, second], ss.at[8], rs.at[8], at_b(1))
                total(3, into_q(2, 1))
                send(q.at[2, :, first], qr.at[:, first], ss.at[9], rs.at[9], at_b(3))

            def across_joined(self):
                waited(qin.at[0], 6)
                qcomb[0] = (q_wide[0] + qin[0].astype(F32)).astype(BF)
                send(qcomb.at[0], ql.at[:, first], ss.at[10], rs.at[10], at_b(1))
                waited(qin.at[1], 7)
                qcomb[1] = (q_wide[1] + qin[1].astype(F32)).astype(BF)
                send(qcomb.at[1], qr.at[:, second], ss.at[11], rs.at[11], at_b(3))

            def result(self):
                here = pl.ds(pl.multiple_of(pb * 48, 16), 48)
                waited(ql.at[:, second], 8)
                waited(qr.at[:, first], 9)
                waited(ql.at[:, first], 10)
                waited(qr.at[:, second], 11)
                return (
                    own[here, :]
                    + from_l[here, :].astype(F32)
                    + from_r[here, :].astype(F32)
                    + ql[...].astype(F32)
                    + qr[...].astype(F32)
                )

        return Stages()

    def small_sum(recv_ref, own_tile, ss, rs):
        acc = own_tile
        for i in range(1, 16):
            remote(recv_ref.at[i], recv_ref.at[i], ss.at[i], rs.at[i], (kv, tp)).wait_recv()
            acc = acc + recv_ref[i]
        return acc

    lane48 = lax.broadcasted_iota(jnp.int32, (48, 128), 1)

    def gate_tiles():
        def step(k, _):
            rows = rows48(k)
            part = jnp.dot(scaled[rows, :], gate_w, preferred_element_type=F32)
            wf = wide[rows, :].astype(F32)
            sq = jnp.sum(wf * wf, axis=1, keepdims=True)
            gsend[k] = transpose_padded(jnp.where(lane48 == 4, sq, part))[:8]
            return 0

        lax.fori_loop(0, 16, step, 0, unroll=4)
        for i in range(1, 16):
            k = kv_peer(i)
            send(gsend.at[k], grecv.at[i], g_s.at[i], g_r.at[i], (k, tp))

    for i in range(1, 5):
        loads[i].wait()
    qk = ring(0, *qk_bufs, qk_s, qk_r)
    vo = ring(NH, *vo_bufs, vo_s, vo_r)
    qk.opposite()
    qk.plain()
    vo.opposite()
    gate_tiles()
    qk.joined()
    vo.plain()
    vo.joined()
    weight_send(0, 1, late, 2, at_a(1))
    weight_send(0, 3, late, 3, at_a(3))
    qk.mine()
    vo.mine()
    qk.across()
    qk.across_joined()
    vo.across()
    gsum = small_sum(grecv, gsend[kv], g_s, g_r)
    inv_row = lax.rsqrt(gsum[4:5, :] / D + EPS)
    inv_col = column_of(inv_row)[:48]
    igate = pair_row(gsum[0:1, :] * inv_row, gsum[1:2, :] * inv_row)
    fpre = pair_row(gsum[2:3, :] * inv_row, gsum[3:4, :] * inv_row) + bias_row
    log_sig = -(jnp.maximum(-fpre, 0.0) + jnp.log1p(jnp.exp(-jnp.abs(fpre))))
    running = forget_row + log_sig
    inter = running + state_row
    pos = lax.broadcasted_iota(jnp.int32, (64, 128), 0).astype(F32)
    tail_log = jnp.where(pos < length_row, running[0:1] + gate_t, -jnp.inf)
    top = jnp.maximum(jnp.maximum(inter[0:1], jnp.max(tail_log, axis=0, keepdims=True)), igate[0:1])
    w_inter = jnp.exp(inter[0:1] - top)
    w_own = column_of(jnp.exp(igate[0:1] - top))
    w_tail = jnp.exp(tail_log - top)

    qk_sum = qk.result()
    for h in range(2):
        qs[h] = qk_sum[:, 128 * h : 128 * h + 128] * inv_col
    for i in range(7, 10):
        loads[i].wait()

    for h in range(2):
        q_hi = qs[h].astype(BF).astype(F32)
        q_lo = (qs[h] - q_hi).astype(BF).astype(F32)
        q_rows[:, 2 * h, :] = q_hi
        q_rows[:, 2 * h + 1, :] = q_lo
    for i in range(4, 8):
        q_rows[:, i, :] = jnp.zeros((48, 128), F32)
    contract_last = (((1,), (1,)), ((), ()))
    lane1 = lax.broadcasted_iota(jnp.int32, (1, 128), 1)

    def recall_step(s, _):
        lhs = q_rows[s].astype(BF)
        state = cbuf[s].reshape(256, 128).astype(BF)
        m = lax.dot_general(lhs, state, contract_last, preferred_element_type=F32)
        mem_n[0, pl.ds(s, 1), :] = m[0:1, :128] + m[1:2, :128]
        mem_n[1, pl.ds(s, 1), :] = m[2:3, 128:] + m[3:4, 128:]
        sc = lax.dot_general(
            lhs, kbuf[s].reshape(128, 128), contract_last, preferred_element_type=F32
        )
        sc_n[pl.ds(s, 1), :] = jnp.where(lane1 < 64, sc[0:1] + sc[1:2], sc[2:3] + sc[3:4])
        return 0

    lax.fori_loop(0, 24, recall_step, 0, unroll=4)
    vo.across_joined()
    lax.fori_loop(24, 48, recall_step, 0, unroll=4)
    sc_r = transpose_padded(sc_n[...])
    sc_t = jnp.where(lane64 < 64, sc_r[:64], pltpu.roll(sc_r[64:], 64, 1))
    weighted = w_tail * (sc_t * 128 ** (-0.5))
    rows_w = jnp.concatenate([weighted, weighted], axis=0).T
    prow = lax.broadcasted_iota(jnp.int32, (128, 256), 0)
    plane = lax.broadcasted_iota(jnp.int32, (128, 256), 1)
    slot = 2 * lax.rem(prow, 2) + lax.div(prow, 64)
    rows_w = jnp.where(lax.div(plane, 64) == slot, jnp.concatenate([rows_w, rows_w], axis=1), 0.0)
    rows_w = rows_w.astype(BF)
    step_of = lax.div(lax.rem(prow, 64), 2)

    def tail_step(g, acc):
        here = jnp.where(step_of == g, 1.0, 0.0).astype(BF)
        vals = vbuf[pl.ds(2 * g, 2)].reshape(256, 128)
        return acc + jnp.dot(rows_w * here, vals, preferred_element_type=F32)

    tail_part = lax.fori_loop(0, 24, tail_step, jnp.zeros((128, 128), F32), unroll=4)
    w_state = column_of(w_inter)
    vo_sum = vo.result()
    mixed = []
    for h in range(2):
        q = qs[h]
        k = qk_sum[:, 256 + 128 * h : 384 + 128 * h] * inv_col * 128 ** (-0.5)
        v = vo_sum[:, 128 * h : 128 * h + 128] * inv_col
        og = vo_sum[:, 256 + 128 * h : 384 + 128 * h] * inv_col
        own = jnp.sum(q * k, axis=1, keepdims=True)
        rows = slice(64 * h, 64 * h + 48)
        recalled = mem_n[h] * w_state[rows] + tail_part[rows] + w_own[rows] * own * v
        ms = jnp.mean(recalled * recalled, axis=1, keepdims=True)
        normed = recalled * lax.rsqrt(ms + EPS)
        hg = head_gain[:, 128 * h : 128 * h + 128]
        mixed.append((normed * hg * (1.0 / (1.0 + jnp.exp(-og)))).astype(BF))
    mix_all[rows48(kv), :] = jnp.concatenate(mixed, axis=1)
    for i in range(1, 16):
        mine = mix_all.at[rows48(kv)]
        send(mine, mine, mix_s.at[i], mix_r.at[i], (kv_peer(i), tp))
    loads[10].wait()
    weight_wait(1, early, 0)
    weight_wait(1, late, 2)
    weight_send(1, 2, (0, 128), 4, at_a(1))
    weight_wait(3, early, 1)
    weight_wait(3, late, 3)
    weight_send(3, 2, (128, 128), 5, at_a(3))
    for i in (1, 3, 4, 12, 5, 7, 13, 15, 2, 8, 6, 9, 11, 14, 10):
        src = mix_all.at[rows48(kv_from(i))]
        remote(src, src, mix_s.at[i], mix_r.at[i], (kv, tp)).wait_recv()
    for r in [4, 3, 5, 2, 6, 1, 7, 0]:
        part = jnp.dot(mix_all[rows96(tp_peer(r)), :], wproj_v[...], preferred_element_type=F32)
        att_send[r] = part.astype(BF)
        if r:
            send(att_send.at[r], att_recv.at[r], att_s.at[r], att_r.at[r], (kv, tp_peer(r)))
    attended = att_send[0].astype(F32)
    for r in range(1, 8):
        remote(att_recv.at[r], att_recv.at[r], att_s.at[r], att_r.at[r], (kv, tp)).wait_recv()
        attended = attended + att_recv[r].astype(F32)
    middle = (wide[rows96(tp), :].astype(F32) + attended).astype(BF)
    mid_all[rows96(tp), :] = middle
    middle_f = middle.astype(F32)
    sm_block = (middle_f * mixer_gain[...]).astype(BF)
    later = []

    def send_unless(here, *args):
        copy = remote(*args)

        @pl.when(jnp.logical_not(here))
        def _():
            copy.start()

        later.append((here, copy))

    for i in range(2):
        sm_own[i] = sm_block[48 * i : 48 * i + 48]
    for n, (dy, dc, i) in enumerate((dy, dc, i) for dy in (2, 1, 3, 0) for dc in range(2) for i in range(2)):
        k = 2 * tp + i
        kz, kx = lax.div(k, 4), lax.rem(k, 4)
        cd = lax.rem(c + dc, 2)
        dev_kv = (1 - cd) * (4 * z + kx) + cd * (4 * kz + x)
        ra = mod4((1 - cd) * (kx + 4 - x) + cd * (kz + 4 - z))
        ib = (1 - cd) * kz + cd * kx
        args = (
            sm_own.at[i], lhs4.at[ra, rows48(ib)], sm_s.at[n], sm_r.at[ra * 4 + ib],
            (dev_kv, 2 * mod4(y + dy) + cd),
        )
        if dy == 0 and dc == 0:
            send_unless(dev_kv == kv, *args)
        else:
            send(*args)
    for i in range(2):
        sq = middle_f[48 * i : 48 * i + 48]
        sq = sq * sq
        row = jnp.sum(transpose_padded(sq[:, :128] + sq[:, 128:]), axis=0, keepdims=True)
        ssend[i] = jnp.broadcast_to(row, (8, 128))
        k = 2 * tp + i
        slot = 4 * mod4(lax.div(k, 4) + 4 - z) + mod4(lax.rem(k, 4) + 4 - x)
        for r in range(8):
            args = (ssend.at[i], srecv.at[slot], sq_s.at[8 * i + r], sq_r.at[slot], (k, tp_peer(r)))
            if r == 0:
                send_unless(k == kv, *args)
            else:
                send(*args)
    def down_weights(slot, part=(0, FFD)):
        return wdown_v.at[pl.ds(part[0], part[1]), pl.ds(256 * slot, 256)]

    def down_send(src_slot, dst_slot, part, i, dev):
        send(down_weights(src_slot, part), down_weights(dst_slot, part), wd_s.at[i], wd_r.at[i], dev)

    def down_got(slot, part, i):
        dst = down_weights(slot, part)
        remote(dst, dst, wd_s.at[i], wd_r.at[i], (kv, tp)).wait_recv()

    whole, upper, lower = (0, FFD), (0, FFD // 2), (FFD // 2, FFD // 2)
    loads[13].wait()
    down_send(0, 1, whole, 0, at_a(1))
    down_send(0, 3, whole, 1, at_a(3))
    for r in [4, 3, 5, 2, 6, 1, 7]:
        mine = mid_all.at[rows96(tp)]
        send(mine, mine, mid_s.at[r], mid_r.at[r], (kv, tp_peer(r)))

    for n in (4, 5):
        weight_wait(2, (128 * (n - 4), 128), n)
    for ra in range(4):
        for ib in range(4):
            dst = lhs4.at[ra, pl.ds(48 * ib, 48)]
            got = remote(dst, dst, sm_s.at[0], sm_r.at[ra * 4 + ib], (kv, tp))
            if ra:
                got.wait_recv()
            else:
                k = kv_of(pa, ib)
                here = lax.div(k, 2) == tp

                @pl.when(jnp.logical_not(here))
                def _():
                    got.wait_recv()

                @pl.when(here)
                def _():
                    lhs4[0, 48 * ib : 48 * ib + 48, :] = sm_own[lax.rem(k, 2)]
    rows_all = jnp.concatenate([lhs4[ra] for ra in range(4)], axis=1)
    first, second = pl.ds(0, FFD), pl.ds(FFD, FFD)

    def half_product(base):
        def step(t, _):
            cols = pl.ds(pl.multiple_of(base + t * 256, 128), 256)
            b_own[:, cols] = jnp.dot(rows_all, wgu[:, cols], preferred_element_type=F32)
            return 0

        lax.fori_loop(0, 5, step, 0, unroll=True)
        cols = pl.ds(base + 1280, 128)
        b_own[:, cols] = jnp.dot(rows_all, wgu[:, cols], preferred_element_type=F32)

    def b_rows(g):
        return pl.ds(pl.multiple_of(mod4(pb + g) * 48, 16), 48)

    def b_put(j, g, cols):
        b_q[j, :, cols] = b_own[b_rows(g), cols].astype(BF)

    def b_wait(dst, i):
        remote(dst, dst, rb_s.at[i], rb_r.at[i], (kv, tp)).wait_recv()

    right, left = at_b(1), at_b(3)
    half_product(0)
    b_put(0, 2, first)
    send(b_q.at[0, :, first], b_qin.at[0], rb_s.at[6], rb_r.at[6], right)
    b_put(2, 3, first)
    send(b_q.at[2, :, first], b_qr.at[:, first], rb_s.at[9], rb_r.at[9], left)
    half_product(FFD)
    b_put(0, 2, second)
    send(b_q.at[0, :, second], b_qin.at[1], rb_s.at[7], rb_r.at[7], left)
    b_put(1, 1, second)
    send(b_q.at[1, :, second], b_ql.at[:, second], rb_s.at[8], rb_r.at[8], right)
    b_wait(b_qin.at[0], 6)
    b_qcomb[0] = (b_own[b_rows(1), first] + b_qin[0].astype(F32)).astype(BF)
    send(b_qcomb.at[0], b_ql.at[:, first], rb_s.at[10], rb_r.at[10], right)
    b_wait(b_qin.at[1], 7)
    b_qcomb[1] = (b_own[b_rows(3), second] + b_qin[1].astype(F32)).astype(BF)
    send(b_qcomb.at[1], b_qr.at[:, second], rb_s.at[11], rb_r.at[11], left)
    for r in range(1, 8):
        src = mid_all.at[rows96(tp_from(r))]
        remote(src, src, mid_s.at[r], mid_r.at[r], (kv, tp)).wait_recv()
    srow = lax.broadcasted_iota(jnp.int32, (32, 256), 0)
    scol = lax.broadcasted_iota(jnp.int32, (32, 256), 1)
    pick = jnp.where(scol == 32 * tp + srow, 1.0, 0.0).astype(BF)
    mid_sel[...] = lax.dot_general(
        pick, mid_all[...], (((1,), (1,)), ((), ())), preferred_element_type=F32
    )
    sq_here = lax.div(kv, 2) == tp
    sq0 = remote(srecv.at[0], srecv.at[0], sq_s.at[0], sq_r.at[0], (kv, tp))

    @pl.when(jnp.logical_not(sq_here))
    def _():
        sq0.wait_recv()

    @pl.when(sq_here)
    def _():
        srecv[0] = ssend[lax.rem(kv, 2)]

    ssum = small_sum(srecv, srecv[0], sq_s, sq_r)
    inv_mid = column_of(lax.rsqrt(ssum[0:1] / D + EPS))[:48]
    b_wait(b_ql.at[:, second], 8)
    b_wait(b_qr.at[:, first], 9)
    b_wait(b_ql.at[:, first], 10)
    b_wait(b_qr.at[:, second], 11)

    def both(cols):
        return b_own[b_rows(0), cols] + b_ql[:, cols].astype(F32) + b_qr[:, cols].astype(F32)

    def hidden_step(t, _):
        cols = pl.ds(pl.multiple_of(t * 128, 128), 128)
        gate = both(cols) * inv_mid
        up = both(pl.ds(pl.multiple_of(t * 128 + FFD, 128), 128)) * inv_mid
        hid[rows48(pb), cols] = (gate * (1.0 / (1.0 + jnp.exp(-gate))) * up).astype(BF)
        return 0

    lax.fori_loop(0, FFD // 128, hidden_step, 0)

    def chunk(rb, part=(0, 48)):
        return hid.at[pl.ds(pl.multiple_of(mod4(pb + 4 - rb) * 48 + part[0], 16), part[1])]

    def hop(ref, i, dev):
        send(ref, ref, h_s.at[i], h_r.at[i], dev)

    def arrived(ref, i):
        remote(ref, ref, h_s.at[i], h_r.at[i], (kv, tp)).wait_recv()

    hop(chunk(0), 0, at_b(1))
    hop(chunk(0), 1, at_b(3))
    down_got(1, whole, 0)
    down_send(1, 2, upper, 2, at_a(1))
    down_got(3, whole, 1)
    down_send(3, 2, lower, 3, at_a(3))
    arrived(chunk(1), 0)
    hop(chunk(1, (0, 32)), 2, at_b(1))
    arrived(chunk(3), 1)
    hop(chunk(3, (32, 16)), 3, at_b(3))
    down_got(2, upper, 2)
    down_got(2, lower, 3)
    arrived(chunk(2, (0, 32)), 2)
    arrived(chunk(2, (32, 16)), 3)

    lane16 = lax.broadcasted_iota(jnp.int32, (8, 16, 128), 2)
    for ra in (2, 1, 3, 0):
        part = jnp.dot(hid[...], wdown_v[:, 256 * ra : 256 * ra + 256], preferred_element_type=F32)
        part = jnp.concatenate([part, jnp.zeros((64, 256), F32)], axis=0).T
        tail = part[:, 128:].reshape(8, 2, 16, 128)
        tail = jnp.where(lane16 < 64, tail[:, 0], pltpu.roll(tail[:, 1], 64, 2))
        fsend[ra, :, 0:32, :] = part[:, :128].reshape(8, 32, 128).astype(BF)
        fsend[ra, :, 32:48, :] = tail.astype(BF)
        for dy in (2, 1, 3, 0):
            for dc in range(2):
                t = 2 * mod4(y + dy) + lax.rem(c + dc, 2)
                if ra or dy or dc:
                    send(
                        fsend.at[ra, t], frecv.at[c, ra, dy], f_s.at[8 * ra + 2 * dy + dc],
                        f_r.at[16 * c + 4 * ra + dy], (kv_of(mod4(pa + 4 - ra), pb), t),
                    )
    frecv[c, 0, 0] = fsend[0, tp]
    other = frecv.at[1 - c, 0, 0]
    remote(other, other, f_s.at[0], f_r.at[16 * (1 - c)], (kv, tp)).wait_recv()
    for cs in range(2):
        mains, tails = [], []
        for ra in range(4):
            piece = 0.0
            for dy in range(4):
                dst = frecv.at[cs, ra, dy]
                if ra or dy:
                    remote(dst, dst, f_s.at[0], f_r.at[16 * cs + 4 * ra + dy], (kv, tp)).wait_recv()
                piece = piece + frecv[cs, ra, dy].astype(F32)
            mains.append(piece[:32])
            tails += [piece[32:], pltpu.roll(piece[32:], 64, 1)]
        by_seq = jnp.concatenate(
            [jnp.concatenate(mains, axis=0).T, jnp.concatenate(tails, axis=0).T[:64]], axis=0
        )
        for ra in range(4):
            block = pltpu.roll(by_seq, (128 - 32 * ra) % 128, 1) if ra else by_seq
            for ib in range(4):
                k = 4 * ib + mod4(x + ra) if cs == 0 else 4 * mod4(z + ra) + ib
                mine = block[48 * ib : 48 * ib + 48]
                if cs == 0:
                    down_rows[rows48(k), :] = mine
                else:
                    down_rows[rows48(k), :] += mine
    for b in range(6):
        cols = slice(128 * b, 128 * b + 128)
        out[:, cols] = (mid_sel[:, cols] + down_rows[cols, :].T[:32]).astype(BF)
    for copy in sends:
        copy.wait_send()
    for here, copy in later:
        @pl.when(jnp.logical_not(here))
        def _():
            copy.wait_send()


def per_device(
    tokens, norm_gain, w_query, w_key, w_value, w_outgate, w_igate, w_fgate, forget_bias, head_gain,
    w_proj, mixer_gain, w_gate, w_up, w_down, state_c, state_m, tail_keys, tail_values, tail_gate,
    block_forget, lengths,
):
    any_spec = pl.BlockSpec(memory_space=pl.ANY)
    vm_spec = pl.BlockSpec(memory_space=pltpu.VMEM)
    dma = pltpu.SemaphoreType.DMA

    def ring_bufs(n):
        return [
            pltpu.VMEM((3, 192, n), BF),
            pltpu.VMEM((192, n), F32),
            pltpu.VMEM((2, 192, n // 2), BF),
            pltpu.VMEM((2, 192, n // 2), BF),
            pltpu.VMEM((192, n), BF),
            pltpu.VMEM((192, n), BF),
            pltpu.VMEM((3, 48, n), BF),
            pltpu.VMEM((2, 48, n // 2), BF),
            pltpu.VMEM((2, 48, n // 2), BF),
            pltpu.VMEM((48, n), BF),
            pltpu.VMEM((48, n), BF),
            pltpu.VMEM((2, 192, n // 2), F32),
            pltpu.VMEM((2, 48, n // 2), F32),
        ]

    scratch = [
        pltpu.VMEM((256, 768), BF),
        pltpu.VMEM((768, 256), BF),
        pltpu.VMEM((768, 256), BF),
        pltpu.VMEM((256, N1), BF),
        pltpu.VMEM((16, 256), BF),
        pltpu.VMEM((16, 256), BF),
        pltpu.VMEM((256, 256), BF),
        pltpu.VMEM((1024, N2), BF),
        pltpu.VMEM((FFD, 1024), BF),
        pltpu.VMEM((48, 2, 128, 128), F32),
        pltpu.VMEM((48, 2, 64, 128), BF),
        pltpu.VMEM((48, 2, 64, 128), BF),
        pltpu.VMEM((16, 8, 128), F32),
        pltpu.VMEM((16, 8, 128), F32),
        pltpu.VMEM((8, 128), F32),
        pltpu.VMEM((128, 128), F32),
        *ring_bufs(NH),
        *ring_bufs(NH),
        pltpu.VMEM((2, 48, 128), F32),
        pltpu.VMEM((48, 8, 128), F32),
        pltpu.VMEM((2, 48, 128), F32),
        pltpu.VMEM((48, 128), F32),
        pltpu.VMEM((768, 256), BF),
        pltpu.VMEM((8, 96, 256), BF),
        pltpu.VMEM((8, 96, 256), BF),
        pltpu.VMEM((768, 256), BF),
        pltpu.VMEM((2, 8, 128), F32),
        pltpu.VMEM((16, 8, 128), F32),
        pltpu.VMEM((32, 768), F32),
        pltpu.VMEM((4, 192, 256), BF),
        pltpu.VMEM((2, 48, 256), BF),
        pltpu.VMEM((192, N2), F32),
        *ring_bufs(N2)[6:11],
        pltpu.VMEM((192, FFD), BF),
        pltpu.VMEM((4, 8, 48, 128), BF),
        pltpu.VMEM((2, 4, 4, 48, 128), BF),
        pltpu.VMEM((768, 128), F32),
        dma((14,)),
        dma((8,)), dma((8,)),
        dma((16,)), dma((16,)),
        dma((16,)), dma((16,)),
        dma((8,)), dma((8,)),
        dma((8,)), dma((8,)),
        dma((16,)), dma((16,)),
        dma((12,)), dma((12,)),
        dma((12,)), dma((12,)),
        dma((12,)), dma((12,)),
        dma((6,)), dma((6,)),
        dma((16,)), dma((16,)),
        dma((4,)), dma((4,)),
        dma((4,)), dma((4,)),
        dma((32,)), dma((32,)),
    ]
    specs = [any_spec] * 21
    for i in (1, 8, 10, 17, 18, 19, 20):
        specs[i] = vm_spec
    specs.append(pl.BlockSpec(memory_space=pltpu.SMEM))
    result_t = pl.pallas_call(
        layer,
        out_shape=jax.ShapeDtypeStruct((32, 768), BF),
        in_specs=specs,
        out_specs=vm_spec,
        scratch_shapes=scratch,
        compiler_params=pltpu.CompilerParams(
            collective_id=0, has_side_effects=True, vmem_limit_bytes=60 * 1024 * 1024
        ),
    )(
        tokens.T, norm_gain.reshape(1, 256), w_query, w_key, w_value, w_outgate, w_igate.T, w_fgate.T,
        head_gain.reshape(1, 256), w_proj, mixer_gain.reshape(1, 256), w_gate, w_up, w_down,
        state_c, tail_keys, tail_values, tail_gate, state_m.T, block_forget.T, lengths.reshape(1, 48), forget_bias,
    )
    return result_t.T


def solution(mesh):
    kvtp = P("kv", "tp")
    return jax.shard_map(
        per_device,
        mesh=mesh,
        in_specs=(
            P(None, ("kv", "tp")), P("kv"), kvtp, kvtp, kvtp, kvtp, P(), P(), P("tp"), P("tp"),
            P("tp", "kv"), P("kv"), kvtp, kvtp, P("tp", "kv"), P("kv", "tp", None, None), kvtp,
            P("kv", "tp", None, None), P("kv", "tp", None, None), P("kv", "tp", None), kvtp, P("kv"),
        ),
        out_specs=P(None, ("kv", "tp")),
        check_vma=False,
    )
```
